32 devices in a mesh: kv: 8 (over z, x), tp: 4 (over y, core).
Axes of the slice: x: 2, y: 2, z: 4, core: 2. Of those that a mesh axis runs over, the one named last changes fastest.
Arguments:
- tokens: bfloat16 [128, 2048], P(None, 'kv'), may hold values from -16 to 16
- norm_gain: bfloat16 [2048], P('kv'), may hold values from 0.099609375 to 1.8984375
- w_query: bfloat16 [2048, 1024], P('kv', 'tp'), may hold values from -0.125 to 0.125
- w_key: bfloat16 [2048, 1024], P('kv', 'tp'), may hold values from -0.125 to 0.125
- w_value: bfloat16 [2048, 2048], P('kv', 'tp'), may hold values from -0.125 to 0.125
- w_gate: bfloat16 [2048, 2048], P('kv', 'tp'), may hold values from -0.125 to 0.125
- w_decay: bfloat16 [2048, 1024], P('kv', 'tp'), may hold values from -0.5 to 0.5
- log_decay: float32 [128, 1024], P('kv', 'tp'), may hold values from -1.5 to 0
- state: float32 [128, 8, 128, 256], P('kv', 'tp'), may hold values from -6 to 6
- out_gain: float32 [256], replicated, may hold values from 0.1 to 1.9
- w_out: bfloat16 [2048, 2048], P('tp', 'kv'), may hold values from -0.125 to 0.125
- mixer_gain: bfloat16 [2048], P('kv'), may hold values from 0.099609375 to 1.8984375
- w_ffgate: bfloat16 [2048, 6144], P('kv', 'tp'), may hold values from -0.125 to 0.125
- w_ffup: bfloat16 [2048, 6144], P('kv', 'tp'), may hold values from -0.125 to 0.125
- w_down: bfloat16 [6144, 2048], P('tp', 'kv'), may hold values from -0.078125 to 0.078125
Outputs:
- result: bfloat16 [128, 2048], P(None, 'kv')
- new_state: float32 [128, 8, 128, 256], P('kv', 'tp')
The draws below stay inside these ranges and needn't reach their ends.
All inputs are finite; a program needn't handle non-finite values.
Results may differ from the reference program's by a relative error of at most 0.028.
Values may be sent and summed in bfloat16 or wider, within the bound.
A program may use at most 64 MiB of HBM per device.

```python
import math
import jax
import jax.numpy as jnp
from jax import lax

D = 2048
HEADS = 8
DK = 128
DV = 256
FF = 6144
BATCH = 128
KW = 1024
VW = 2048
N_TP = 4


def draw_tokens(key, part):
    base = jnp.clip(jax.random.normal(jax.random.fold_in(key, 11), (BATCH, D), jnp.float32), -4.0, 4.0)
    rough = jax.random.uniform(jax.random.fold_in(key, 12), (1, D), jnp.float32, 0.5, 1.5)
    ramp = jnp.exp(jnp.linspace(0.0, math.log(6.0), D))[None, :]
    values = base * ramp * rough / 2.5
    return jnp.clip(values, -16.0, 16.0).astype(jnp.bfloat16)


def steps_of(key, shape, cuts, smallest, largest):
    def one(dim, shards_of):
        draws = jax.random.uniform(jax.random.fold_in(jax.random.fold_in(key, 6), dim), (shards_of,), jnp.float32, smallest / len(cuts), largest / len(cuts))
        return jnp.repeat(jnp.exp(draws), shape[dim] // shards_of).reshape((-1,) + (1,) * (len(shape) - dim - 1))

    loudness = one(*cuts[0])
    for cut in cuts[1:]:
        loudness = loudness * one(*cut)
    return loudness


def noise(own_key, dims, deviation, limit, shards=(), dtype=jnp.bfloat16):
    array = deviation * jax.random.normal(own_key, dims, jnp.float32)
    if shards:
        array = array * steps_of(own_key, dims, shards, -0.22, 0.18)
    return jnp.clip(array, -limit, limit).astype(dtype)


def setup_inputs(seed: int = 0) -> dict:
    arg_keys = jax.random.split(jax.random.key(seed), 16)
    tokens = draw_tokens(jax.random.fold_in(arg_keys[15], 71), 0)
    norm_gain = jnp.clip(1.0 + 0.18 * jax.random.normal(arg_keys[1], (D,), jnp.float32), 0.099609375, 1.8984375).astype(jnp.bfloat16)
    w_query = noise(arg_keys[2], (D, KW), D ** -0.5, 0.125, ((0, 8), (1, 4)))
    w_key = noise(arg_keys[3], (D, KW), D ** -0.5, 0.125, ((0, 8), (1, 4)))
    w_value = noise(arg_keys[4], (D, VW), D ** -0.5, 0.125, ((0, 8), (1, 4)))
    w_gate = noise(arg_keys[5], (D, VW), D ** -0.5, 0.125, ((0, 8), (1, 4)))
    w_decay = noise(arg_keys[6], (D, KW), (D // 16) ** -0.5, 0.5, ((0, 8), (1, 4)))
    log_decay = jnp.clip(-1.5 + 1.5 * jax.random.uniform(arg_keys[7], (BATCH, KW), jnp.float32) ** steps_of(arg_keys[7], (BATCH, KW), ((0, 8), (1, 4)), -0.2, 0.2), -1.5, 0.0)
    state = noise(arg_keys[8], (BATCH, HEADS, DK, DV), 1.0, 6.0, ((0, 8), (1, 4)), jnp.float32)
    out_gain = jnp.clip(1.0 + 0.18 * jax.random.normal(arg_keys[9], (DV,), jnp.float32), 0.1, 1.9)
    w_out = noise(arg_keys[10], (VW, D), VW ** -0.5, 0.125, ((0, 4), (1, 8)))
    mixer_gain = jnp.clip(1.0 + 0.18 * jax.random.normal(arg_keys[11], (D,), jnp.float32), 0.099609375, 1.8984375).astype(jnp.bfloat16)
    w_ffgate = noise(arg_keys[12], (D, FF), D ** -0.5, 0.125, ((0, 8), (1, 4)))
    w_ffup = noise(arg_keys[13], (D, FF), D ** -0.5, 0.125, ((0, 8), (1, 4)))
    w_down = noise(arg_keys[14], (FF, D), FF ** -0.5, 0.078125, ((0, 4), (1, 8)))
    return dict(tokens=tokens, norm_gain=norm_gain, w_query=w_query, w_key=w_key, w_value=w_value, w_gate=w_gate, w_decay=w_decay, log_decay=log_decay, state=state, out_gain=out_gain, w_out=w_out, mixer_gain=mixer_gain, w_ffgate=w_ffgate, w_ffup=w_ffup, w_down=w_down)


eps = 1e-06
gate_norm = 16.0

def group_sum(left, right, groups):
    width = left.shape[1] // groups
    total = jnp.zeros((left.shape[0], right.shape[1]), jnp.float32)
    for group in range(groups):
        part = jnp.dot(left[:, group * width:(group + 1) * width], right[group * width:(group + 1) * width], preferred_element_type=jnp.float32)
        part = lax.optimization_barrier(part.astype(jnp.bfloat16))
        total = total + part.astype(jnp.float32)
    return total

def reference(tokens, norm_gain, w_query, w_key, w_value, w_gate, w_decay, log_decay, state, out_gain, w_out, mixer_gain, w_ffgate, w_ffup, w_down):
    wide = tokens.astype(jnp.float32)
    scaled = (wide * norm_gain.astype(jnp.float32)).astype(jnp.bfloat16)
    inv = lax.rsqrt(lax.optimization_barrier(jnp.mean(wide * wide, axis=1, keepdims=True)) + eps)
    query = jnp.dot(scaled, w_query, preferred_element_type=jnp.float32) * inv
    key = jnp.dot(scaled, w_key, preferred_element_type=jnp.float32) * inv
    value = jnp.dot(scaled, w_value, preferred_element_type=jnp.float32) * inv
    gate = jnp.dot(scaled, w_gate, preferred_element_type=jnp.float32) * inv
    decay_pre = jnp.dot(scaled, w_decay, preferred_element_type=jnp.float32) * inv
    log_a = jax.nn.log_sigmoid(decay_pre) / gate_norm + log_decay
    query = query.reshape(BATCH, HEADS, DK) * DK ** (-0.5)
    key = key.reshape(BATCH, HEADS, DK)
    value = value.reshape(BATCH, HEADS, DV)
    new_state = state * jnp.exp(log_a).reshape(BATCH, HEADS, DK)[..., None] + key[..., None] * value[:, :, None, :]
    attended = jnp.einsum('bhk,bhkv->bhv', query, new_state, precision=lax.Precision.HIGHEST)
    normed = attended * lax.rsqrt(lax.optimization_barrier(jnp.mean(attended * attended, axis=2, keepdims=True)) + eps) * out_gain
    mixed = (normed.reshape(BATCH, VW) * jax.nn.silu(gate)).astype(jnp.bfloat16)
    attn_sum = group_sum(mixed, w_out, N_TP)
    middle = (wide + attn_sum).astype(jnp.bfloat16)
    wide2 = middle.astype(jnp.float32)
    scaled2 = (wide2 * mixer_gain.astype(jnp.float32)).astype(jnp.bfloat16)
    inv2 = lax.rsqrt(lax.optimization_barrier(jnp.mean(wide2 * wide2, axis=1, keepdims=True)) + eps)
    gate2 = jnp.dot(scaled2, w_ffgate, preferred_element_type=jnp.float32) * inv2
    upper = jnp.dot(scaled2, w_ffup, preferred_element_type=jnp.float32) * inv2
    hidden = (jax.nn.silu(gate2) * upper).astype(jnp.bfloat16)
    down_sum = group_sum(hidden, w_down, N_TP)
    result = (wide2 + down_sum).astype(jnp.bfloat16)
    return (result, new_state)
```

```python
import functools

import jax
import jax.numpy as jnp
from jax import lax
from jax.experimental import pallas as pl
from jax.experimental.pallas import tpu as pltpu
from jax.sharding import PartitionSpec as P

eps = 1e-06
gate_norm = 16.0
LANES = 128
SUBLANES = 8
FF_SIZES = (1, 1, 2, 2, 2, 2, 1)
LAG_Z = 0
LAG_X = 2
AX, AZ, BZ, BX, CY, DX, DZ, EZ, EX, FY, SQX, SQZ, PHASES = 0, 1, 2, 3, 4, 5, 6, 7, 8, 9, 10, 12, 14
F32 = jnp.float32
BF16 = jnp.bfloat16


def remote(src, dst, send_sem, recv_sem, device):
    return pltpu.make_async_remote_copy(
        src_ref=src,
        dst_ref=dst,
        send_sem=send_sem,
        recv_sem=recv_sem,
        device_id=device,
        device_id_type=pl.DeviceIdType.MESH,
    )


def split_axis(n_kv):
    n_in = 1
    while n_in * n_in * 4 <= n_kv:
        n_in *= 2
    return n_kv // n_in, n_in


def ff_chunks(width):
    if width % LANES:
        return [(0, width)]
    left, sizes, k = width // LANES, [], 0
    while left:
        take = min(left, FF_SIZES[min(k, len(FF_SIZES) - 1)])
        sizes.append(take)
        left -= take
        k += 1
    at, ranges = 0, []
    for take in sizes:
        ranges.append((at, at + take * LANES))
        at += take * LANES
    return ranges


def proj_layout(kw, vw, dk, dv):
    heads = kw // dk
    at, chunks, where = 0, [], []

    def put(items):
        nonlocal at
        pieces, places = [], []
        for weight, lo, width in items:
            pieces.append((weight, lo, width, at))
            places.append(at)
            at += width
        chunks.append(pieces)
        return places

    for h in range(heads):
        q, k = put([("q", h * dk, dk), ("k", h * dk, dk)])
        d, v = put([("d", h * dk, dk), ("v", h * dv, dv)])
        where.append((q, k, d, v))
    (g,) = put([("g", 0, vw)])
    return chunks, where, g, at


def kernel(
    n_kv,
    n_tp,
    d_model,
    tokens_hbm,
    norm_gain_hbm,
    wq_hbm,
    wk_hbm,
    wv_hbm,
    wg_hbm,
    wd_hbm,
    log_decay_hbm,
    state_hbm,
    out_gain_hbm,
    wo_hbm,
    mixer_gain_hbm,
    wfg_hbm,
    wfu_hbm,
    wdn_hbm,
    result_ref,
    ns_ref,
    tokens_ref,
    norm_gain_ref,
    log_decay_ref,
    out_gain_ref,
    mixer_gain_ref,
    wall,
    wo,
    wff,
    wdn,
    sqx,
    sqz,
    px,
    rx,
    pz,
    rz,
    att,
    mg,
    to,
    fx,
    frx,
    fz,
    frz,
    hg,
    td,
    middle_ref,
    in_sem,
    w_sem,
    bulk_sem,
    send_sem,
    sq_r,
    ax_r,
    az_r,
    mz_r,
    t_r,
    fx_r,
    fz_r,
    hz_r,
    hx_r,
):
    n_out, n_in = split_axis(n_kv)
    kv = lax.axis_index("kv")
    tp = lax.axis_index("tp")
    zi = kv // n_in
    xi = lax.rem(kv, n_in)
    rows = px.shape[2]
    batch, feats = tokens_ref.shape
    heads, dk, dv = ns_ref.shape[1:]
    kw = wq_hbm.shape[1]
    vw = wv_hbm.shape[1]
    ff = wfg_hbm.shape[1]

    def x_peer(d):
        return lax.rem(xi + d, n_in)

    def z_peer(d):
        return lax.rem(zi + d, n_out)

    def z_back(d):
        return lax.rem(zi + n_out - d, n_out)

    def x_dev(d):
        return (zi * n_in + x_peer(d), tp)

    def z_dev(d):
        return (z_peer(d) * n_in + xi, tp)

    def t_dev(d):
        return (kv, lax.rem(tp + d, n_tp))

    barrier = pltpu.get_barrier_semaphore()
    peers = (
        [z_dev(d) for d in range(1, n_out)]
        + [x_dev(d) for d in range(1, n_in)]
        + [t_dev(d) for d in range(1, n_tp)]
    )
    for dev in peers:
        pl.semaphore_signal(barrier, inc=1, device_id=dev, device_id_type=pl.DeviceIdType.MESH)

    def fetch(src, dst, sem):
        copy = pltpu.make_async_copy(src, dst, sem)
        copy.start()
        return copy

    chunks, where, g_at, width = proj_layout(kw, vw, dk, dv)
    source = {"q": wq_hbm, "k": wk_hbm, "d": wd_hbm, "v": wv_hbm, "g": wg_hbm}
    first_loads = [
        fetch(tokens_hbm, tokens_ref, in_sem.at[0]),
        fetch(norm_gain_hbm, norm_gain_ref, in_sem.at[1]),
    ]
    bounds = []
    for c, pieces in enumerate(chunks):
        for name, lo, wide, at in pieces:
            fetch(source[name].at[:, lo : lo + wide], wall.at[:, at : at + wide], w_sem.at[c])
        bounds.append((pieces[0][3], pieces[-1][3] + pieces[-1][2]))

    def took(ref, sem):
        pltpu.make_async_copy(ref, ref, sem).wait()

    def launch(phase, src, dst, recv_sem, device):
        remote(src, dst, send_sem.at[phase], recv_sem, device).start()

    def scatter_rows(dst, value, lo):
        wide = value.shape[1]
        value = value.astype(BF16)
        for z in range(n_out):
            for x in range(n_in):
                at = (z * n_in + x) * rows
                dst[x, z, :, lo : lo + wide] = value[at : at + rows]

    def send_x(phase, src, dst, sem, lo, hi):
        for d in range(1, n_in):
            launch(
                phase,
                src.at[x_peer(d), :, :, lo:hi],
                dst.at[d - 1, :, :, lo:hi],
                sem,
                x_dev(d),
            )

    def send_z(phase, src, dst, sem, lo, hi):
        for d in range(1, n_out):
            launch(
                phase,
                src.at[z_peer(d), :, lo:hi],
                dst.at[d - 1, :, lo:hi],
                sem,
                z_dev(d),
            )

    def reduce_x(src, got, dst, sem, lo, hi):
        total = src[xi, :, :, lo:hi].astype(F32)
        if n_in > 1:
            took(got.at[:, :, :, lo:hi], sem)
            for d in range(1, n_in):
                total = total + got[d - 1, :, :, lo:hi].astype(F32)
        dst[:, :, lo:hi] = total.astype(BF16)

    def reduce_z(src, got, sem, lo, hi):
        total = src[zi, :, lo:hi].astype(F32)
        if n_out > 1:
            took(got.at[:, :, lo:hi], sem)
            for d in range(1, n_out):
                total = total + got[d - 1, :, lo:hi].astype(F32)
        return total

    def squares_x(i, values):
        ones = jnp.ones((SUBLANES, feats), F32)
        sqx[i, 0] = lax.dot_general(
            ones,
            values * values,
            (((1,), (1,)), ((), ())),
            precision=lax.Precision.HIGHEST,
            preferred_element_type=F32,
        )
        for d in range(1, n_in):
            launch(SQX + i, sqx.at[i, 0], sqx.at[i, d], sq_r.at[i, 0], x_dev(d))

    def squares_z(i):
        if n_in > 1:
            took(sqx.at[i, 1:n_in], sq_r.at[i, 0])
        total = sqx[i, 0]
        for d in range(1, n_in):
            total = total + sqx[i, d]
        sqz[i, 0] = total
        for d in range(1, n_out):
            launch(SQZ + i, sqz.at[i, 0], sqz.at[i, d], sq_r.at[i, 1], z_dev(d))

    def inverse(i):
        if n_out > 1:
            took(sqz.at[i, 1:n_out], sq_r.at[i, 1])
        total = sqz[i, 0]
        for d in range(1, n_out):
            total = total + sqz[i, d]
        lane = lax.broadcasted_iota(jnp.int32, (rows, batch), 1)
        mine = lax.broadcasted_iota(jnp.int32, (rows, batch), 0) + kv * rows
        own = jnp.where(lane == mine, jnp.broadcast_to(total[:1], (rows, batch)), 0.0)
        return lax.rsqrt(jnp.sum(own, axis=1, keepdims=True) / d_model + eps)

    for load in first_loads:
        load.wait()
    wide = tokens_ref[...].astype(F32)
    scaled = (wide * norm_gain_ref[...].astype(F32).reshape(1, -1)).astype(BF16)

    for c, (lo, hi) in enumerate(bounds):
        took(wall.at[:, lo:hi], w_sem.at[c])
        scatter_rows(px, jnp.dot(scaled, wall[:, lo:hi], preferred_element_type=F32), lo)
        if c == 0:
            pl.semaphore_wait(barrier, len(peers))
        send_x(AX, px, rx, ax_r.at[c], lo, hi)
        if c == 0:
            squares_x(0, wide)
    load_decay = fetch(log_decay_hbm, log_decay_ref, in_sem.at[0])
    load_gain = fetch(out_gain_hbm, out_gain_ref, in_sem.at[1])
    load_mixer = fetch(mixer_gain_hbm, mixer_gain_ref, in_sem.at[2])
    load_state = fetch(state_hbm, ns_ref, bulk_sem.at[0])
    load_o = fetch(wo_hbm, wo, bulk_sem.at[1])
    fchunks = ff_chunks(ff)
    n_c = len(fchunks)
    fbounds = [(2 * lo, 2 * hi) for lo, hi in fchunks]
    for lo, hi in fchunks:
        fetch(wfg_hbm.at[:, lo:hi], wff.at[:, 2 * lo : lo + hi], bulk_sem.at[2])
        fetch(wfu_hbm.at[:, lo:hi], wff.at[:, lo + hi : 2 * hi], bulk_sem.at[2])
    load_dn = fetch(wdn_hbm, wdn, bulk_sem.at[3])

    for c, (lo, hi) in enumerate(bounds):
        reduce_x(px, rx, pz, ax_r.at[c], lo, hi)
        send_z(AZ, pz, rz, az_r.at[c], lo, hi)
        if c == 0:
            squares_z(0)

    load_decay.wait()
    load_state.wait()
    inv = None
    for h in range(heads):
        c = 2 * h
        q_at, k_at, d_at, v_at = (at for at in where[h])
        qk = reduce_z(pz, rz, az_r.at[c], *bounds[c])
        if h == 0:
            inv = inverse(0)
        qk = qk * inv
        dv_terms = reduce_z(pz, rz, az_r.at[c + 1], *bounds[c + 1]) * inv
        query = qk[:, :dk] * dk ** (-0.5)
        pre = dv_terms[:, :dk]
        values = dv_terms[:, dk:]
        log_sig = jnp.minimum(pre, 0.0) - jnp.log1p(jnp.exp(-jnp.abs(pre)))
        decay = jnp.exp(log_sig / gate_norm + log_decay_ref[:, h * dk : (h + 1) * dk])
        q_t = query.T
        k_t = qk[:, dk:].T
        a_t = decay.T
        for b in range(rows):
            col = slice(b, b + 1)
            new = ns_ref[b, h] * a_t[:, col] + k_t[:, col] * values[col, :]
            ns_ref[b, h] = new
            att[h, col, :] = jnp.sum(new * q_t[:, col], axis=0, keepdims=True)

    load_gain.wait()
    last = len(bounds) - 1
    gate = reduce_z(pz, rz, az_r.at[last], *bounds[last]) * inv
    for h in range(heads):
        got = att[h]
        normed = (
            got
            * lax.rsqrt(jnp.mean(got * got, axis=1, keepdims=True) + eps)
            * out_gain_ref[...]
        )
        cols = slice(h * dv, (h + 1) * dv)
        mg[zi, xi, :, cols] = (normed * jax.nn.silu(gate[:, cols])).astype(BF16)

    own = mg.at[zi, xi]
    for d in range(1, n_out):
        launch(BZ, own, own, mz_r.at[d - 1], z_dev(d))
    for dz in range(n_out):
        slot = mg.at[z_back(dz), xi]
        if dz:
            took(slot, mz_r.at[dz - 1])
        for d in range(1, n_in):
            launch(BX, slot, slot, t_r.at[2], x_dev(d))
    load_o.wait()
    if n_in > 1:
        took(mg.at[:, : n_in - 1], t_r.at[2])

    def sum_groups(phase, buf, sem):
        for d in range(1, n_tp):
            launch(phase, buf.at[tp], buf.at[tp], sem, t_dev(d))
        if n_tp > 1:
            took(buf.at[: n_tp - 1], sem)
        total = buf[0].astype(F32)
        for g in range(1, n_tp):
            total = total + buf[g].astype(F32)
        return total

    mixed = mg[...].reshape(batch, vw)
    to[tp] = jnp.dot(mixed, wo[...], preferred_element_type=F32).astype(BF16)
    middle = (tokens_ref[...].astype(F32) + sum_groups(CY, to, t_r.at[0])).astype(BF16)
    middle_ref[...] = middle

    load_mixer.wait()
    wide2 = middle.astype(F32)
    scaled2 = (wide2 * mixer_gain_ref[...].astype(F32).reshape(1, -1)).astype(BF16)
    took(wff, bulk_sem.at[2])
    for c, (lo, hi) in enumerate(fbounds):
        scatter_rows(fx, jnp.dot(scaled2, wff[:, lo:hi], preferred_element_type=F32), lo)
        send_x(DX, fx, frx, fx_r.at[c], lo, hi)
        if c == 0:
            squares_x(1, wide2)

    inv2 = [None]

    def to_z(c):
        lo, hi = fbounds[c]
        reduce_x(fx, frx, fz, fx_r.at[c], lo, hi)
        send_z(DZ, fz, frz, fz_r.at[c], lo, hi)
        if c == 0:
            squares_z(1)

    def activate(c):
        terms = reduce_z(fz, frz, fz_r.at[c], *fbounds[c])
        if c == 0:
            inv2[0] = inverse(1)
        terms = terms * inv2[0]
        fc = terms.shape[1] // 2
        cols = slice(*fchunks[c])
        hg[zi, xi, :, cols] = (jax.nn.silu(terms[:, :fc]) * terms[:, fc:]).astype(BF16)
        own = hg.at[zi, xi, :, cols]
        for d in range(1, n_out):
            launch(EZ, own, own, hz_r.at[c], z_dev(d))

    def hand_on(c):
        cols = slice(*fchunks[c])
        if n_out > 1:
            took(hg.at[: n_out - 1, 0, :, cols], hz_r.at[c])
        slot = hg.at[:, xi, :, cols]
        for d in range(1, n_in):
            launch(EX, slot, slot, hx_r.at[c], x_dev(d))

    lag_z = n_c + LAG_Z
    lag_x = lag_z + LAG_X
    for t in range(n_c + lag_x):
        if t < n_c:
            to_z(t)
        if 0 <= t - lag_z < n_c:
            activate(t - lag_z)
        if 0 <= t - lag_x < n_c:
            hand_on(t - lag_x)

    load_dn.wait()
    down = None
    for c, (lo, hi) in enumerate(fchunks):
        if n_in > 1:
            took(hg.at[:, : n_in - 1, :, lo:hi], hx_r.at[c])
        term = jnp.dot(
            hg[:, :, :, lo:hi].reshape(batch, hi - lo),
            wdn[lo:hi, :],
            preferred_element_type=F32,
        )
        down = term if down is None else down + term
    td[tp] = down.astype(BF16)
    total = sum_groups(FY, td, t_r.at[1])
    result_ref[...] = (middle_ref[...].astype(F32) + total).astype(BF16)

    if n_in > 1:
        took(rx, send_sem.at[AX])
        took(frx, send_sem.at[DX])
        took(mg.at[:, : n_in - 1], send_sem.at[BX])
        took(hg.at[:, : n_in - 1], send_sem.at[EX])
        for i in range(2):
            took(sqx.at[i, 1:n_in], send_sem.at[SQX + i])
    if n_out > 1:
        took(rz, send_sem.at[AZ])
        took(frz, send_sem.at[DZ])
        took(mg.at[: n_out - 1, 0], send_sem.at[BZ])
        took(hg.at[: n_out - 1, 0], send_sem.at[EZ])
        for i in range(2):
            took(sqz.at[i, 1:n_out], send_sem.at[SQZ + i])
    if n_tp > 1:
        took(to.at[: n_tp - 1], send_sem.at[CY])
        took(td.at[: n_tp - 1], send_sem.at[FY])


def body(n_kv, n_tp, *args):
    (
        tokens,
        norm_gain,
        w_query,
        w_key,
        w_value,
        w_gate,
        w_decay,
        log_decay,
        state,
        out_gain,
        w_out,
        mixer_gain,
        w_ffgate,
        w_ffup,
        w_down,
    ) = args
    n_out, n_in = split_axis(n_kv)
    batch, feats = tokens.shape
    rows, heads, dk, dv = state.shape
    kw = w_query.shape[1]
    vw = w_value.shape[1]
    ff = w_ffgate.shape[1]
    n_c = len(ff_chunks(ff))
    chunks, _, _, width = proj_layout(kw, vw, dk, dv)
    n_a = len(chunks)
    m_in, m_out = max(n_in - 1, 1), max(n_out - 1, 1)
    dma = pltpu.SemaphoreType.DMA
    vmem = pltpu.VMEM
    whole = pl.BlockSpec(memory_space=pltpu.VMEM)
    far = pl.BlockSpec(memory_space=pl.ANY)
    sems = [
        (3,),
        (n_a,),
        (4,),
        (PHASES,),
        (2, 2),
        (n_a,),
        (n_a,),
        (m_out,),
        (3,),
        (n_c,),
        (n_c,),
        (n_c,),
        (n_c,),
    ]
    result, new_state = pl.pallas_call(
        functools.partial(kernel, n_kv, n_tp, feats * n_kv),
        out_shape=(
            vmem((batch, feats), BF16),
            vmem(state.shape, F32),
        ),
        in_specs=[far] * 15,
        out_specs=(whole, whole),
        scratch_shapes=[
            vmem((batch, feats), BF16),
            vmem(norm_gain.shape, BF16),
            vmem(log_decay.shape, F32),
            vmem((1, dv), F32),
            vmem(mixer_gain.shape, BF16),
            vmem((feats, width), BF16),
            vmem(w_out.shape, BF16),
            vmem((feats, 2 * ff), BF16),
            vmem(w_down.shape, BF16),
            vmem((2, n_in, SUBLANES, batch), F32),
            vmem((2, n_out, SUBLANES, batch), F32),
            vmem((n_in, n_out, rows, width), BF16),
            vmem((m_in, n_out, rows, width), BF16),
            vmem((n_out, rows, width), BF16),
            vmem((m_out, rows, width), BF16),
            vmem((heads, rows, dv), F32),
            vmem((n_out, n_in, rows, vw), BF16),
            vmem((n_tp, batch, feats), BF16),
            vmem((n_in, n_out, rows, 2 * ff), BF16),
            vmem((m_in, n_out, rows, 2 * ff), BF16),
            vmem((n_out, rows, 2 * ff), BF16),
            vmem((m_out, rows, 2 * ff), BF16),
            vmem((n_out, n_in, rows, ff), BF16),
            vmem((n_tp, batch, feats), BF16),
            vmem((batch, feats), BF16),
        ]
        + [dma(shape) for shape in sems],
        compiler_params=pltpu.CompilerParams(
            collective_id=0, has_side_effects=True, vmem_limit_bytes=56 * 2**20
        ),
    )(
        tokens,
        norm_gain,
        w_query,
        w_key,
        w_value,
        w_gate,
        w_decay,
        log_decay,
        state,
        out_gain.reshape(1, dv),
        w_out,
        mixer_gain,
        w_ffgate,
        w_ffup,
        w_down,
    )
    return (result, new_state)


def solution(mesh):
    return jax.shard_map(
        functools.partial(body, mesh.shape["kv"], mesh.shape["tp"]),
        mesh=mesh,
        in_specs=(
            P(None, "kv"),
            P("kv"),
            P("kv", "tp"),
            P("kv", "tp"),
            P("kv", "tp"),
            P("kv", "tp"),
            P("kv", "tp"),
            P("kv", "tp"),
            P("kv", "tp", None, None),
            P(),
            P("tp", "kv"),
            P("kv"),
            P("kv", "tp"),
            P("kv", "tp"),
            P("tp", "kv"),
        ),
        out_specs=(P(None, "kv"), P("kv", "tp", None, None)),
        check_vma=False,
    )
```

```python
import functools

import jax
import jax.numpy as jnp
from jax import lax
from jax.experimental import pallas as pl
from jax.experimental.pallas import tpu as pltpu
from jax.sharding import PartitionSpec as P

eps = 1e-06
gate_norm = 16.0
LANES = 128
SUBLANES = 8
FF_SIZES = (1, 1, 2, 2, 2, 1)
FF_Z = 2
LAG_ZX = 7
SQ_AT = 1
A_ZF = 1
LAG_ZACT = 11
LAG_ACT = 9
LAG_RELAY = 50
LAG_HAND = 100
DIRECT = 99
AX, AZ, BZ, BX, CY, DX, DZ, EZ, EX, FY, SQX, SQZ, ZF, XF, PHASES = 0, 1, 2, 3, 4, 5, 6, 7, 8, 9, 10, 12, 14, 16, 18
F32 = jnp.float32
BF16 = jnp.bfloat16


def remote(src, dst, send_sem, recv_sem, device):
    return pltpu.make_async_remote_copy(
        src_ref=src,
        dst_ref=dst,
        send_sem=send_sem,
        recv_sem=recv_sem,
        device_id=device,
        device_id_type=pl.DeviceIdType.MESH,
    )


def split_axis(n_kv):
    n_in = 1
    while n_in * n_in * 4 <= n_kv:
        n_in *= 2
    return n_kv // n_in, n_in


def ff_chunks(width, z_units):
    if width % LANES:
        return [(0, width)]
    units = width // LANES
    tail = z_units if z_units < units else 0
    left, sizes, k = units - tail, [], 0
    while left:
        take = min(left, FF_SIZES[min(k, len(FF_SIZES) - 1)])
        sizes.append(take)
        left -= take
        k += 1
    if tail:
        sizes.append(tail)
    at, ranges = 0, []
    for take in sizes:
        ranges.append((at, at + take * LANES))
        at += take * LANES
    return ranges


def proj_layout(kw, vw, dk, dv):
    heads = kw // dk
    at, chunks, where = 0, [], []

    def put(items):
        nonlocal at
        pieces, places = [], []
        for weight, lo, width in items:
            pieces.append((weight, lo, width, at))
            places.append(at)
            at += width
        chunks.append(pieces)
        return places

    for h in range(heads):
        q, k = put([("q", h * dk, dk), ("k", h * dk, dk)])
        d, v = put([("d", h * dk, dk), ("v", h * dv, dv)])
        where.append((q, k, d, v))
    (g,) = put([("g", 0, vw)])
    return chunks, where, g, at


def kernel(
    n_kv,
    n_tp,
    d_model,
    tokens_hbm,
    norm_gain_hbm,
    wq_hbm,
    wk_hbm,
    wv_hbm,
    wg_hbm,
    wd_hbm,
    log_decay_hbm,
    state_hbm,
    out_gain_hbm,
    wo_hbm,
    mixer_gain_hbm,
    wfg_hbm,
    wfu_hbm,
    wdn_hbm,
    result_ref,
    ns_ref,
    tokens_ref,
    norm_gain_ref,
    log_decay_ref,
    out_gain_ref,
    mixer_gain_ref,
    wall,
    wo,
    wff,
    wdn,
    sqx,
    sqz,
    px,
    rx,
    pz,
    rz,
    att,
    mg,
    to,
    away,
    fx,
    frx,
    fz,
    frz,
    hg,
    td,
    middle_ref,
    zfr,
    zfs,
    zfx,
    dfr,
    dfs,
    dfx,
    in_sem,
    w_sem,
    bulk_sem,
    send_sem,
    sq_r,
    ax_r,
    az_r,
    mz_r,
    t_r,
    fx_r,
    fz_r,
    hz_r,
    hp_r,
    hx_r,
    zf_r,
):
    n_out, n_in = split_axis(n_kv)
    kv = lax.axis_index("kv")
    tp = lax.axis_index("tp")
    zi = kv // n_in
    xi = lax.rem(kv, n_in)
    rows = px.shape[2]
    batch, feats = tokens_ref.shape
    heads, dk, dv = ns_ref.shape[1:]
    kw = wq_hbm.shape[1]
    vw = wv_hbm.shape[1]
    ff = wfg_hbm.shape[1]

    def x_peer(d):
        return lax.rem(xi + d, n_in)

    def z_peer(d):
        return lax.rem(zi + d, n_out)

    def z_back(d):
        return lax.rem(zi + n_out - d, n_out)

    def x_dev(d):
        return (zi * n_in + x_peer(d), tp)

    def z_dev(d):
        return (z_peer(d) * n_in + xi, tp)

    def t_dev(d):
        return (kv, lax.rem(tp + d, n_tp))

    def xt_dev(d, e):
        return (zi * n_in + x_peer(d), lax.rem(tp + e, n_tp))

    barrier = pltpu.get_barrier_semaphore()
    peers = [z_dev(d) for d in range(1, n_out)] + [
        xt_dev(d, e) for d in range(n_in) for e in range(n_tp) if d or e
    ]
    for dev in peers:
        pl.semaphore_signal(barrier, inc=1, device_id=dev, device_id_type=pl.DeviceIdType.MESH)

    def fetch(src, dst, sem):
        copy = pltpu.make_async_copy(src, dst, sem)
        copy.start()
        return copy

    chunks, where, g_at, width = proj_layout(kw, vw, dk, dv)
    source = {"q": wq_hbm, "k": wk_hbm, "d": wd_hbm, "v": wv_hbm, "g": wg_hbm}
    first_loads = [
        fetch(tokens_hbm, tokens_ref, in_sem.at[0]),
        fetch(norm_gain_hbm, norm_gain_ref, in_sem.at[1]),
    ]
    bounds = []
    two_way = n_in > 1 and n_out > 1
    a_zf = 2 * (heads - 1) if two_way and A_ZF else None
    order = [0] + sorted(range(1, len(chunks)), key=lambda c: (c != a_zf, c))
    for c in order:
        for name, lo, wide, at in chunks[c]:
            fetch(source[name].at[:, lo : lo + wide], wall.at[:, at : at + wide], w_sem.at[c])
    for pieces in chunks:
        bounds.append((pieces[0][3], pieces[-1][3] + pieces[-1][2]))

    def took(ref, sem):
        pltpu.make_async_copy(ref, ref, sem).wait()

    def launch(phase, src, dst, recv_sem, device):
        remote(src, dst, send_sem.at[phase], recv_sem, device).start()

    def scatter_rows(dst, value, lo):
        wide = value.shape[1]
        value = value.astype(BF16)
        for z in range(n_out):
            for x in range(n_in):
                at = (z * n_in + x) * rows
                dst[x, z, :, lo : lo + wide] = value[at : at + rows]

    def send_x(phase, src, dst, sem, lo, hi):
        for d in range(1, n_in):
            launch(
                phase,
                src.at[x_peer(d), :, :, lo:hi],
                dst.at[d - 1, :, :, lo:hi],
                sem,
                x_dev(d),
            )

    def send_z(phase, src, dst, sem, lo, hi):
        for d in range(1, n_out):
            launch(
                phase,
                src.at[z_peer(d), :, lo:hi],
                dst.at[d - 1, :, lo:hi],
                sem,
                z_dev(d),
            )

    def reduce_x(src, got, dst, sem, lo, hi):
        total = src[xi, :, :, lo:hi].astype(F32)
        if n_in > 1:
            took(got.at[:, :, :, lo:hi], sem)
            for d in range(1, n_in):
                total = total + got[d - 1, :, :, lo:hi].astype(F32)
        dst[:, :, lo:hi] = total.astype(BF16)

    def reduce_z(src, got, sem, lo, hi):
        total = src[zi, :, lo:hi].astype(F32)
        if n_out > 1:
            took(got.at[:, :, lo:hi], sem)
            for d in range(1, n_out):
                total = total + got[d - 1, :, lo:hi].astype(F32)
        return total

    def zf_send(i, src, dst, lo, hi):
        for d in range(1, n_out):
            launch(ZF + i, src.at[:, z_peer(d), :, lo:hi], dst.at[d - 1], zf_r.at[i, 0], z_dev(d))

    def zf_to_x(i, src, got, mid, dst, lo, hi):
        took(got, zf_r.at[i, 0])
        total = src[:, zi, :, lo:hi].astype(F32)
        for d in range(1, n_out):
            total = total + got[d - 1].astype(F32)
        mid[...] = total.astype(BF16)
        for d in range(1, n_in):
            launch(XF + i, mid.at[x_peer(d)], dst.at[d - 1], zf_r.at[i, 1], x_dev(d))

    def zf_final(i, mid, got):
        took(got, zf_r.at[i, 1])
        total = mid[xi].astype(F32)
        for d in range(1, n_in):
            total = total + got[d - 1].astype(F32)
        return total

    def squares_x(i, values):
        ones = jnp.ones((SUBLANES, feats), F32)
        sqx[i, 0] = lax.dot_general(
            ones,
            values * values,
            (((1,), (1,)), ((), ())),
            precision=lax.Precision.HIGHEST,
            preferred_element_type=F32,
        )
        for d in range(1, n_in):
            launch(SQX + i, sqx.at[i, 0], sqx.at[i, d], sq_r.at[i, 0], x_dev(d))

    def squares_z(i):
        if n_in > 1:
            took(sqx.at[i, 1:n_in], sq_r.at[i, 0])
        total = sqx[i, 0]
        for d in range(1, n_in):
            total = total + sqx[i, d]
        sqz[i, 0] = total
        for d in range(1, n_out):
            launch(SQZ + i, sqz.at[i, 0], sqz.at[i, d], sq_r.at[i, 1], z_dev(d))

    def inverse(i):
        if n_out > 1:
            took(sqz.at[i, 1:n_out], sq_r.at[i, 1])
        total = sqz[i, 0]
        for d in range(1, n_out):
            total = total + sqz[i, d]
        lane = lax.broadcasted_iota(jnp.int32, (rows, batch), 1)
        mine = lax.broadcasted_iota(jnp.int32, (rows, batch), 0) + kv * rows
        own = jnp.where(lane == mine, jnp.broadcast_to(total[:1], (rows, batch)), 0.0)
        return lax.rsqrt(jnp.sum(own, axis=1, keepdims=True) / d_model + eps)

    for load in first_loads:
        load.wait()
    wide = tokens_ref[...].astype(F32)
    scaled = (wide * norm_gain_ref[...].astype(F32).reshape(1, -1)).astype(BF16)

    for k, c in enumerate(order):
        lo, hi = bounds[c]
        took(wall.at[:, lo:hi], w_sem.at[c])
        scatter_rows(px, jnp.dot(scaled, wall[:, lo:hi], preferred_element_type=F32), lo)
        if k == 0:
            pl.semaphore_wait(barrier, len(peers))
        if c == a_zf:
            zf_send(0, px, zfr, lo, hi)
        else:
            send_x(AX, px, rx, ax_r.at[c], lo, hi)
        if k == 1:
            squares_x(0, wide)
    load_decay = fetch(log_decay_hbm, log_decay_ref, in_sem.at[0])
    load_gain = fetch(out_gain_hbm, out_gain_ref, in_sem.at[1])
    load_mixer = fetch(mixer_gain_hbm, mixer_gain_ref, in_sem.at[2])
    load_state = fetch(state_hbm, ns_ref, bulk_sem.at[0])
    load_o = fetch(wo_hbm, wo.at[xi], bulk_sem.at[1])
    fchunks = ff_chunks(ff, FF_Z if two_way else 0)
    n_c = len(fchunks)
    d_zf = n_c - 1 if two_way and n_c > 1 else None
    fbounds = [(2 * lo, 2 * hi) for lo, hi in fchunks]
    for lo, hi in fchunks:
        fetch(wfg_hbm.at[:, lo:hi], wff.at[:, 2 * lo : lo + hi], bulk_sem.at[2])
        fetch(wfu_hbm.at[:, lo:hi], wff.at[:, lo + hi : 2 * hi], bulk_sem.at[2])
    load_dn = fetch(wdn_hbm, wdn, bulk_sem.at[3])

    x_order = [c for c in order if c != a_zf]
    for k, c in enumerate(x_order):
        lo, hi = bounds[c]
        if a_zf is not None and k == len(x_order) - 1:
            zf_to_x(0, px, zfr, zfs, zfx, *bounds[a_zf])
        reduce_x(px, rx, pz, ax_r.at[c], lo, hi)
        send_z(AZ, pz, rz, az_r.at[c], lo, hi)
        if k == 1:
            squares_z(0)

    for d in range(1, n_in):
        launch(BX, wo_hbm, wo.at[xi], t_r.at[2], x_dev(d))

    def arrived(c):
        if c == a_zf:
            return zf_final(0, zfs, zfx)
        return reduce_z(pz, rz, az_r.at[c], *bounds[c])


    load_decay.wait()
    load_state.wait()
    inv = None
    for h in range(heads):
        c = 2 * h
        q_at, k_at, d_at, v_at = (at for at in where[h])
        qk = arrived(c)
        if h == 0:
            inv = inverse(0)
        qk = qk * inv
        dv_terms = arrived(c + 1) * inv
        query = qk[:, :dk] * dk ** (-0.5)
        pre = dv_terms[:, :dk]
        values = dv_terms[:, dk:]
        log_sig = jnp.minimum(pre, 0.0) - jnp.log1p(jnp.exp(-jnp.abs(pre)))
        decay = jnp.exp(log_sig / gate_norm + log_decay_ref[:, h * dk : (h + 1) * dk])
        q_t = query.T
        k_t = qk[:, dk:].T
        a_t = decay.T
        for b in range(rows):
            col = slice(b, b + 1)
            new = ns_ref[b, h] * a_t[:, col] + k_t[:, col] * values[col, :]
            ns_ref[b, h] = new
            att[h, col, :] = jnp.sum(new * q_t[:, col], axis=0, keepdims=True)

    load_gain.wait()
    last = len(bounds) - 1
    gate = reduce_z(pz, rz, az_r.at[last], *bounds[last]) * inv
    for h in range(heads):
        got = att[h]
        normed = (
            got
            * lax.rsqrt(jnp.mean(got * got, axis=1, keepdims=True) + eps)
            * out_gain_ref[...]
        )
        cols = slice(h * dv, (h + 1) * dv)
        mg[zi, :, cols] = (normed * jax.nn.silu(gate[:, cols])).astype(BF16)

    own = mg.at[zi]
    for d in range(1, n_out):
        launch(BZ, own, own, mz_r.at[0], z_dev(d))
    load_o.wait()
    if n_in > 1:
        took(wo.at[: n_in - 1], t_r.at[2])
    if n_out > 1:
        took(mg.at[: n_out - 1], mz_r.at[0])
    mixed = mg[...].reshape(n_out * rows, vw)
    mine = xi * n_tp + tp
    for d in range(1, n_in):
        part = jnp.dot(mixed, wo[x_peer(d)], preferred_element_type=F32)
        away[d - 1] = part.astype(BF16)
        for e in range(n_tp):
            launch(CY, away.at[d - 1], to.at[mine], t_r.at[3], xt_dev(d, e))
    to[mine] = jnp.dot(mixed, wo[xi], preferred_element_type=F32).astype(BF16)
    for e in range(1, n_tp):
        launch(CY, to.at[mine], to.at[mine], t_r.at[0], t_dev(e))

    def heads_sum(x):
        total = to[x * n_tp].astype(F32)
        for g in range(1, n_tp):
            total = total + to[x * n_tp + g].astype(F32)
        tok = jnp.stack(
            [tokens_ref[pl.ds((z * n_in + x) * rows, rows), :] for z in range(n_out)]
        )
        return (tok.astype(F32) + total.reshape(n_out, rows, feats)).astype(BF16)

    if n_tp > 1:
        took(to.at[: n_tp - 1], t_r.at[0])
    middle_ref[:, xi] = heads_sum(xi)
    if n_in > 1:
        took(to.at[: (n_in - 1) * n_tp], t_r.at[3])
    for d in range(1, n_in):
        middle_ref[:, x_peer(d)] = heads_sum(x_peer(d))
    middle = middle_ref[...].reshape(batch, feats)

    def sum_groups(phase, buf, sem):
        for d in range(1, n_tp):
            launch(phase, buf.at[tp], buf.at[tp], sem, t_dev(d))
        if n_tp > 1:
            took(buf.at[: n_tp - 1], sem)
        total = buf[0].astype(F32)
        for g in range(1, n_tp):
            total = total + buf[g].astype(F32)
        return total

    load_mixer.wait()
    wide2 = middle.astype(F32)
    scaled2 = (wide2 * mixer_gain_ref[...].astype(F32).reshape(1, -1)).astype(BF16)
    took(wff, bulk_sem.at[2])
    d_order = list(range(n_c))
    if d_zf is not None:
        d_order = [0, d_zf] + list(range(1, d_zf))
    for k, c in enumerate(d_order):
        lo, hi = fbounds[c]
        scatter_rows(fx, jnp.dot(scaled2, wff[:, lo:hi], preferred_element_type=F32), lo)
        if c == d_zf:
            zf_send(1, fx, dfr, lo, hi)
        else:
            send_x(DX, fx, frx, fx_r.at[c], lo, hi)
        if k == min(SQ_AT, n_c - 1):
            squares_x(1, wide2)

    inv2 = [None]
    half = n_out // 2

    def relayed(c):
        return n_out % 2 == 0 and c < n_c - DIRECT

    def near_dev(d):
        base = (zi // half) * half
        return ((base + lax.rem(zi - base + d, half)) * n_in + xi, tp)

    def to_z(c):
        lo, hi = fbounds[c]
        reduce_x(fx, frx, fz, fx_r.at[c], lo, hi)
        send_z(DZ, fz, frz, fz_r.at[c], lo, hi)
        if c == min(1, n_c - 2):
            squares_z(1)

    def activate(c):
        if c == d_zf:
            terms = zf_final(1, dfs, dfx)
        else:
            terms = reduce_z(fz, frz, fz_r.at[c], *fbounds[c])
        if inv2[0] is None:
            inv2[0] = inverse(1)
        terms = terms * inv2[0]
        fc = terms.shape[1] // 2
        cols = slice(*fchunks[c])
        hg[zi, xi, :, cols] = (jax.nn.silu(terms[:, :fc]) * terms[:, fc:]).astype(BF16)
        own = hg.at[zi, xi, :, cols]
        if not relayed(c):
            for d in range(1, n_out):
                launch(EZ, own, own, hz_r.at[c], z_dev(d))
            return
        for d in range(1, half):
            launch(EZ, own, own, hz_r.at[c], near_dev(d))
        launch(EZ, own, own, hp_r.at[c], z_dev(half))

    def relay(c):
        if not relayed(c):
            return
        cols = slice(*fchunks[c])
        slot = hg.at[z_peer(half), xi, :, cols]
        took(slot, hp_r.at[c])
        for d in range(1, half):
            launch(EZ, slot, slot, hz_r.at[c], near_dev(d))

    def hand_on(c):
        cols = slice(*fchunks[c])
        far = 2 * (half - 1) if relayed(c) else n_out - 1
        if far:
            took(hg.at[:far, 0, :, cols], hz_r.at[c])
        slot = hg.at[:, xi, :, cols]
        for d in range(1, n_in):
            launch(EX, slot, slot, hx_r.at[c], x_dev(d))

    steps = []
    for c in range(n_c):
        at = fchunks[c][1] / LANES
        if c == d_zf:
            steps.append((LAG_ZX, len(steps), lambda c: zf_to_x(1, fx, dfr, dfs, dfx, *fbounds[c]), c))
            steps.append((LAG_ZACT, len(steps), activate, c))
        else:
            steps.append((at, len(steps), to_z, c))
            steps.append((at + LAG_ACT, len(steps), activate, c))
        steps.append((at + LAG_RELAY, len(steps), relay, c))
        steps.append((at + LAG_HAND if c != d_zf else LAG_HAND, len(steps), hand_on, c))
    for _, _, step, c in sorted(steps, key=lambda item: item[:2]):
        step(c)

    load_dn.wait()
    down = None
    for c, (lo, hi) in enumerate(fchunks):
        if n_in > 1:
            took(hg.at[:, : n_in - 1, :, lo:hi], hx_r.at[c])
        term = jnp.dot(
            hg[:, :, :, lo:hi].reshape(batch, hi - lo),
            wdn[lo:hi, :],
            preferred_element_type=F32,
        )
        down = term if down is None else down + term
    td[tp] = down.astype(BF16)
    total = sum_groups(FY, td, t_r.at[1])
    wide3 = middle_ref[...].reshape(batch, feats).astype(F32)
    result_ref[...] = (wide3 + total).astype(BF16)

    def sent_but(ref, phase, ranges, but):
        left = sum(hi - lo for c, (lo, hi) in enumerate(ranges) if c != but)
        took(ref.at[..., :left], send_sem.at[phase])

    if a_zf is not None:
        took(zfr, send_sem.at[ZF])
        took(zfx, send_sem.at[XF])
    if d_zf is not None:
        took(dfr, send_sem.at[ZF + 1])
        took(dfx, send_sem.at[XF + 1])
    if n_in > 1:
        sent_but(rx, AX, bounds, a_zf)
        sent_but(frx, DX, fbounds, d_zf)
        took(wo.at[: n_in - 1], send_sem.at[BX])
        took(hg.at[:, : n_in - 1], send_sem.at[EX])
        for i in range(2):
            took(sqx.at[i, 1:n_in], send_sem.at[SQX + i])
    if n_out > 1:
        sent_but(rz, AZ, bounds, a_zf)
        sent_but(frz, DZ, fbounds, d_zf)
        took(mg.at[: n_out - 1], send_sem.at[BZ])
        took(hg.at[: n_out - 1, 0], send_sem.at[EZ])
        for i in range(2):
            took(sqz.at[i, 1:n_out], send_sem.at[SQZ + i])
    if n_in * n_tp > 1:
        took(to.at[: n_in * n_tp - 1], send_sem.at[CY])
    if n_tp > 1:
        took(td.at[: n_tp - 1], send_sem.at[FY])


def body(n_kv, n_tp, *args):
    (
        tokens,
        norm_gain,
        w_query,
        w_key,
        w_value,
        w_gate,
        w_decay,
        log_decay,
        state,
        out_gain,
        w_out,
        mixer_gain,
        w_ffgate,
        w_ffup,
        w_down,
    ) = args
    n_out, n_in = split_axis(n_kv)
    batch, feats = tokens.shape
    rows, heads, dk, dv = state.shape
    kw = w_query.shape[1]
    vw = w_value.shape[1]
    ff = w_ffgate.shape[1]
    n_in_out = n_in > 1 and n_out > 1
    fchunks = ff_chunks(ff, FF_Z if n_in_out else 0)
    n_c = len(fchunks)
    d_w = 2 * (fchunks[-1][1] - fchunks[-1][0])
    a_w = 2 * dk
    chunks, _, _, width = proj_layout(kw, vw, dk, dv)
    n_a = len(chunks)
    m_in, m_out = max(n_in - 1, 1), max(n_out - 1, 1)
    dma = pltpu.SemaphoreType.DMA
    vmem = pltpu.VMEM
    whole = pl.BlockSpec(memory_space=pltpu.VMEM)
    far = pl.BlockSpec(memory_space=pl.ANY)
    sems = [
        (3,),
        (n_a,),
        (4,),
        (PHASES,),
        (2, 2),
        (n_a,),
        (n_a,),
        (1,),
        (4,),
        (n_c,),
        (n_c,),
        (n_c,),
        (n_c,),
        (n_c,),
        (2, 2),
    ]
    result, new_state = pl.pallas_call(
        functools.partial(kernel, n_kv, n_tp, feats * n_kv),
        out_shape=(
            vmem((batch, feats), BF16),
            vmem(state.shape, F32),
        ),
        in_specs=[far] * 15,
        out_specs=(whole, whole),
        scratch_shapes=[
            vmem((batch, feats), BF16),
            vmem(norm_gain.shape, BF16),
            vmem(log_decay.shape, F32),
            vmem((1, dv), F32),
            vmem(mixer_gain.shape, BF16),
            vmem((feats, width), BF16),
            vmem((n_in,) + w_out.shape, BF16),
            vmem((feats, 2 * ff), BF16),
            vmem(w_down.shape, BF16),
            vmem((2, n_in, SUBLANES, batch), F32),
            vmem((2, n_out, SUBLANES, batch), F32),
            vmem((n_in, n_out, rows, width), BF16),
            vmem((m_in, n_out, rows, width), BF16),
            vmem((n_out, rows, width), BF16),
            vmem((m_out, rows, width), BF16),
            vmem((heads, rows, dv), F32),
            vmem((n_out, rows, vw), BF16),
            vmem((n_in * n_tp, n_out * rows, feats), BF16),
            vmem((m_in, n_out * rows, feats), BF16),
            vmem((n_in, n_out, rows, 2 * ff), BF16),
            vmem((m_in, n_out, rows, 2 * ff), BF16),
            vmem((n_out, rows, 2 * ff), BF16),
            vmem((m_out, rows, 2 * ff), BF16),
            vmem((n_out, n_in, rows, ff), BF16),
            vmem((n_tp, batch, feats), BF16),
            vmem((n_out, n_in, rows, feats), BF16),
            vmem((m_out, n_in, rows, a_w), BF16),
            vmem((n_in, rows, a_w), BF16),
            vmem((m_in, rows, a_w), BF16),
            vmem((m_out, n_in, rows, d_w), BF16),
            vmem((n_in, rows, d_w), BF16),
            vmem((m_in, rows, d_w), BF16),
        ]
        + [dma(shape) for shape in sems],
        compiler_params=pltpu.CompilerParams(
            collective_id=0, has_side_effects=True, vmem_limit_bytes=56 * 2**20
        ),
    )(
        tokens,
        norm_gain,
        w_query,
        w_key,
        w_value,
        w_gate,
        w_decay,
        log_decay,
        state,
        out_gain.reshape(1, dv),
        w_out,
        mixer_gain,
        w_ffgate,
        w_ffup,
        w_down,
    )
    return (result, new_state)


def solution(mesh):
    return jax.shard_map(
        functools.partial(body, mesh.shape["kv"], mesh.shape["tp"]),
        mesh=mesh,
        in_specs=(
            P(None, "kv"),
            P("kv"),
            P("kv", "tp"),
            P("kv", "tp"),
            P("kv", "tp"),
            P("kv", "tp"),
            P("kv", "tp"),
            P("kv", "tp"),
            P("kv", "tp", None, None),
            P(),
            P("tp", "kv"),
            P("kv"),
            P("kv", "tp"),
            P("kv", "tp"),
            P("tp", "kv"),
        ),
        out_specs=(P(None, "kv"), P("kv", "tp", None, None)),
        check_vma=False,
    )
```

```python
import functools

import jax
import jax.numpy as jnp
from jax import lax
from jax.experimental import pallas as pl
from jax.experimental.pallas import tpu as pltpu
from jax.sharding import PartitionSpec as P

eps = 1e-06
gate_norm = 16.0
LANES = 128
SUBLANES = 8
FF_SIZES = (1,)
FF_Z = 2
LAG_ZX = 8
SQ_AT = 1
A_SQ = 0
A_SQZ = 0
SQ_Z = 0
A_ZF = 1
LAG_ZACT = 12
LAG_ACT = 11
LAG_HAND = 100
LAG_ZHAND = 100
AX, AZ, BZ, BX, CY, DX, DZ, EZ, EX, FY, SQX, SQZ, ZF, XF, PHASES = 0, 1, 2, 3, 4, 5, 6, 7, 8, 9, 10, 12, 14, 16, 18
F32 = jnp.float32
BF16 = jnp.bfloat16


def remote(src, dst, send_sem, recv_sem, device):
    return pltpu.make_async_remote_copy(
        src_ref=src,
        dst_ref=dst,
        send_sem=send_sem,
        recv_sem=recv_sem,
        device_id=device,
        device_id_type=pl.DeviceIdType.MESH,
    )


def split_axis(n_kv):
    n_in = 1
    while n_in * n_in * 4 <= n_kv:
        n_in *= 2
    return n_kv // n_in, n_in


def ff_chunks(width, z_units):
    if width % LANES:
        return [(0, width)]
    units = width // LANES
    tail = z_units if z_units < units else 0
    left, sizes, k = units - tail, [], 0
    while left:
        take = min(left, FF_SIZES[min(k, len(FF_SIZES) - 1)])
        sizes.append(take)
        left -= take
        k += 1
    if tail:
        sizes.append(tail)
    at, ranges = 0, []
    for take in sizes:
        ranges.append((at, at + take * LANES))
        at += take * LANES
    return ranges


def proj_layout(kw, vw, dk, dv):
    heads = kw // dk
    at, chunks, where = 0, [], []

    def put(items):
        nonlocal at
        pieces, places = [], []
        for weight, lo, width in items:
            pieces.append((weight, lo, width, at))
            places.append(at)
            at += width
        chunks.append(pieces)
        return places

    for h in range(heads):
        q, k = put([("q", h * dk, dk), ("k", h * dk, dk)])
        d, v = put([("d", h * dk, dk), ("v", h * dv, dv)])
        where.append((q, k, d, v))
    (g,) = put([("g", 0, vw)])
    return chunks, where, g, at


def kernel(
    n_kv,
    n_tp,
    d_model,
    tokens_hbm,
    norm_gain_hbm,
    wq_hbm,
    wk_hbm,
    wv_hbm,
    wg_hbm,
    wd_hbm,
    log_decay_hbm,
    state_hbm,
    out_gain_hbm,
    wo_hbm,
    mixer_gain_hbm,
    wfg_hbm,
    wfu_hbm,
    wdn_hbm,
    result_ref,
    ns_ref,
    tokens_ref,
    norm_gain_ref,
    log_decay_ref,
    out_gain_ref,
    mixer_gain_ref,
    wall,
    wo,
    wff,
    wdn,
    sqx,
    sqz,
    px,
    rx,
    pz,
    rz,
    att,
    mg,
    to,
    away,
    fx,
    frx,
    fz,
    frz,
    hg,
    td,
    middle_ref,
    zfr,
    zfs,
    zfx,
    dfr,
    dfs,
    dfx,
    in_sem,
    w_sem,
    bulk_sem,
    send_sem,
    sq_r,
    ax_r,
    az_r,
    mz_r,
    t_r,
    fx_r,
    fz_r,
    hz_r,
    hx_r,
    zf_r,
):
    n_out, n_in = split_axis(n_kv)
    kv = lax.axis_index("kv")
    tp = lax.axis_index("tp")
    zi = kv // n_in
    xi = lax.rem(kv, n_in)
    rows = px.shape[2]
    batch, feats = tokens_ref.shape
    heads, dk, dv = ns_ref.shape[1:]
    kw = wq_hbm.shape[1]
    vw = wv_hbm.shape[1]
    ff = wfg_hbm.shape[1]

    def x_peer(d):
        return lax.rem(xi + d, n_in)

    def z_peer(d):
        return lax.rem(zi + d, n_out)

    def z_back(d):
        return lax.rem(zi + n_out - d, n_out)

    def x_dev(d):
        return (zi * n_in + x_peer(d), tp)

    def z_dev(d):
        return (z_peer(d) * n_in + xi, tp)

    def t_dev(d):
        return (kv, lax.rem(tp + d, n_tp))

    def xt_dev(d, e):
        return (zi * n_in + x_peer(d), lax.rem(tp + e, n_tp))

    barrier = pltpu.get_barrier_semaphore()
    peers = [z_dev(d) for d in range(1, n_out)] + [
        xt_dev(d, e) for d in range(n_in) for e in range(n_tp) if d or e
    ]
    for dev in peers:
        pl.semaphore_signal(barrier, inc=1, device_id=dev, device_id_type=pl.DeviceIdType.MESH)

    def fetch(src, dst, sem):
        copy = pltpu.make_async_copy(src, dst, sem)
        copy.start()
        return copy

    chunks, where, g_at, width = proj_layout(kw, vw, dk, dv)
    source = {"q": wq_hbm, "k": wk_hbm, "d": wd_hbm, "v": wv_hbm, "g": wg_hbm}
    first_loads = [
        fetch(tokens_hbm, tokens_ref, in_sem.at[0]),
        fetch(norm_gain_hbm, norm_gain_ref, in_sem.at[1]),
    ]
    bounds = []
    two_way = n_in > 1 and n_out > 1
    a_zf = 2 * (heads - 1) if two_way and A_ZF else None
    order = [0] + sorted(range(1, len(chunks)), key=lambda c: (c != a_zf, c))
    for c in order:
        for name, lo, wide, at in chunks[c]:
            fetch(source[name].at[:, lo : lo + wide], wall.at[:, at : at + wide], w_sem.at[c])
    for pieces in chunks:
        bounds.append((pieces[0][3], pieces[-1][3] + pieces[-1][2]))

    def took(ref, sem):
        pltpu.make_async_copy(ref, ref, sem).wait()

    def launch(phase, src, dst, recv_sem, device):
        remote(src, dst, send_sem.at[phase], recv_sem, device).start()

    def scatter_rows(dst, value, lo):
        wide = value.shape[1]
        value = value.astype(BF16)
        for z in range(n_out):
            for x in range(n_in):
                at = (z * n_in + x) * rows
                dst[x, z, :, lo : lo + wide] = value[at : at + rows]

    def send_x(phase, src, dst, sem, lo, hi):
        for d in range(1, n_in):
            launch(
                phase,
                src.at[x_peer(d), :, :, lo:hi],
                dst.at[d - 1, :, :, lo:hi],
                sem,
                x_dev(d),
            )

    def send_z(phase, src, dst, sem, lo, hi):
        for d in range(1, n_out):
            launch(
                phase,
                src.at[z_peer(d), :, lo:hi],
                dst.at[d - 1, :, lo:hi],
                sem,
                z_dev(d),
            )

    def reduce_x(src, got, dst, sem, lo, hi):
        total = src[xi, :, :, lo:hi].astype(F32)
        if n_in > 1:
            took(got.at[:, :, :, lo:hi], sem)
            for d in range(1, n_in):
                total = total + got[d - 1, :, :, lo:hi].astype(F32)
        dst[:, :, lo:hi] = total.astype(BF16)

    def reduce_z(src, got, sem, lo, hi):
        total = src[zi, :, lo:hi].astype(F32)
        if n_out > 1:
            took(got.at[:, :, lo:hi], sem)
            for d in range(1, n_out):
                total = total + got[d - 1, :, lo:hi].astype(F32)
        return total

    def zf_send(i, src, dst, lo, hi):
        for d in range(1, n_out):
            launch(ZF + i, src.at[:, z_peer(d), :, lo:hi], dst.at[d - 1], zf_r.at[i, 0], z_dev(d))

    def zf_to_x(i, src, got, mid, dst, lo, hi):
        took(got, zf_r.at[i, 0])
        total = src[:, zi, :, lo:hi].astype(F32)
        for d in range(1, n_out):
            total = total + got[d - 1].astype(F32)
        mid[...] = total.astype(BF16)
        for d in range(1, n_in):
            launch(XF + i, mid.at[x_peer(d)], dst.at[d - 1], zf_r.at[i, 1], x_dev(d))

    def zf_final(i, mid, got):
        took(got, zf_r.at[i, 1])
        total = mid[xi].astype(F32)
        for d in range(1, n_in):
            total = total + got[d - 1].astype(F32)
        return total

    def squares_x(i, values):
        ones = jnp.ones((SUBLANES, feats), F32)
        sqx[i, 0] = lax.dot_general(
            ones,
            values * values,
            (((1,), (1,)), ((), ())),
            precision=lax.Precision.HIGHEST,
            preferred_element_type=F32,
        )
        for d in range(1, n_in):
            launch(SQX + i, sqx.at[i, 0], sqx.at[i, d], sq_r.at[i, 0], x_dev(d))

    def squares_z(i):
        if n_in > 1:
            took(sqx.at[i, 1:n_in], sq_r.at[i, 0])
        total = sqx[i, 0]
        for d in range(1, n_in):
            total = total + sqx[i, d]
        sqz[i, 0] = total
        for d in range(1, n_out):
            launch(SQZ + i, sqz.at[i, 0], sqz.at[i, d], sq_r.at[i, 1], z_dev(d))

    def inverse(i):
        if n_out > 1:
            took(sqz.at[i, 1:n_out], sq_r.at[i, 1])
        total = sqz[i, 0]
        for d in range(1, n_out):
            total = total + sqz[i, d]
        lane = lax.broadcasted_iota(jnp.int32, (rows, batch), 1)
        mine = lax.broadcasted_iota(jnp.int32, (rows, batch), 0) + kv * rows
        own = jnp.where(lane == mine, jnp.broadcast_to(total[:1], (rows, batch)), 0.0)
        return lax.rsqrt(jnp.sum(own, axis=1, keepdims=True) / d_model + eps)

    for load in first_loads:
        load.wait()
    wide = tokens_ref[...].astype(F32)
    scaled = (wide * norm_gain_ref[...].astype(F32).reshape(1, -1)).astype(BF16)

    for k, c in enumerate(order):
        lo, hi = bounds[c]
        took(wall.at[:, lo:hi], w_sem.at[c])
        scatter_rows(px, jnp.dot(scaled, wall[:, lo:hi], preferred_element_type=F32), lo)
        if k == 0:
            pl.semaphore_wait(barrier, len(peers))
        if c == a_zf:
            zf_send(0, px, zfr, lo, hi)
        else:
            send_x(AX, px, rx, ax_r.at[c], lo, hi)
        if k == A_SQ:
            squares_x(0, wide)
    load_decay = fetch(log_decay_hbm, log_decay_ref, in_sem.at[0])
    load_gain = fetch(out_gain_hbm, out_gain_ref, in_sem.at[1])
    load_mixer = fetch(mixer_gain_hbm, mixer_gain_ref, in_sem.at[2])
    load_state = fetch(state_hbm, ns_ref, bulk_sem.at[0])
    load_o = fetch(wo_hbm, wo.at[xi], bulk_sem.at[1])
    fchunks = ff_chunks(ff, FF_Z if two_way else 0)
    n_c = len(fchunks)
    d_zf = n_c - 1 if two_way and n_c > 1 else None
    fbounds = [(2 * lo, 2 * hi) for lo, hi in fchunks]
    for lo, hi in fchunks:
        fetch(wfg_hbm.at[:, lo:hi], wff.at[:, 2 * lo : lo + hi], bulk_sem.at[2])
        fetch(wfu_hbm.at[:, lo:hi], wff.at[:, lo + hi : 2 * hi], bulk_sem.at[2])
    load_dn = fetch(wdn_hbm, wdn, bulk_sem.at[3])

    x_order = [c for c in order if c != a_zf]
    for k, c in enumerate(x_order):
        lo, hi = bounds[c]
        if a_zf is not None and k == len(x_order) - 1:
            zf_to_x(0, px, zfr, zfs, zfx, *bounds[a_zf])
        reduce_x(px, rx, pz, ax_r.at[c], lo, hi)
        send_z(AZ, pz, rz, az_r.at[c], lo, hi)
        if k == A_SQZ:
            squares_z(0)

    for d in range(1, n_in):
        launch(BX, wo_hbm, wo.at[xi], t_r.at[2], x_dev(d))

    def arrived(c):
        if c == a_zf:
            return zf_final(0, zfs, zfx)
        return reduce_z(pz, rz, az_r.at[c], *bounds[c])


    load_decay.wait()
    load_state.wait()
    inv = None
    for h in range(heads):
        c = 2 * h
        q_at, k_at, d_at, v_at = (at for at in where[h])
        qk = arrived(c)
        if h == 0:
            inv = inverse(0)
        qk = qk * inv
        dv_terms = arrived(c + 1) * inv
        query = qk[:, :dk] * dk ** (-0.5)
        pre = dv_terms[:, :dk]
        values = dv_terms[:, dk:]
        log_sig = jnp.minimum(pre, 0.0) - jnp.log1p(jnp.exp(-jnp.abs(pre)))
        decay = jnp.exp(log_sig / gate_norm + log_decay_ref[:, h * dk : (h + 1) * dk])
        q_t = query.T
        k_t = qk[:, dk:].T
        a_t = decay.T
        for b in range(rows):
            col = slice(b, b + 1)
            new = ns_ref[b, h] * a_t[:, col] + k_t[:, col] * values[col, :]
            ns_ref[b, h] = new
            att[h, col, :] = jnp.sum(new * q_t[:, col], axis=0, keepdims=True)

    load_gain.wait()
    last = len(bounds) - 1
    gate = reduce_z(pz, rz, az_r.at[last], *bounds[last]) * inv
    for h in range(heads):
        got = att[h]
        normed = (
            got
            * lax.rsqrt(jnp.mean(got * got, axis=1, keepdims=True) + eps)
            * out_gain_ref[...]
        )
        cols = slice(h * dv, (h + 1) * dv)
        mg[zi, :, cols] = (normed * jax.nn.silu(gate[:, cols])).astype(BF16)

    own = mg.at[zi]
    for d in range(1, n_out):
        launch(BZ, own, own, mz_r.at[0], z_dev(d))
    load_o.wait()
    if n_in > 1:
        took(wo.at[: n_in - 1], t_r.at[2])
    if n_out > 1:
        took(mg.at[: n_out - 1], mz_r.at[0])
    mixed = mg[...].reshape(n_out * rows, vw)
    mine = xi * n_tp + tp
    for d in range(1, n_in):
        part = jnp.dot(mixed, wo[x_peer(d)], preferred_element_type=F32)
        away[d - 1] = part.astype(BF16)
        for e in range(n_tp):
            launch(CY, away.at[d - 1], to.at[mine], t_r.at[3], xt_dev(d, e))
    to[mine] = jnp.dot(mixed, wo[xi], preferred_element_type=F32).astype(BF16)
    for e in range(1, n_tp):
        launch(CY, to.at[mine], to.at[mine], t_r.at[0], t_dev(e))

    def heads_sum(x):
        total = to[x * n_tp].astype(F32)
        for g in range(1, n_tp):
            total = total + to[x * n_tp + g].astype(F32)
        tok = jnp.stack(
            [tokens_ref[pl.ds((z * n_in + x) * rows, rows), :] for z in range(n_out)]
        )
        return (tok.astype(F32) + total.reshape(n_out, rows, feats)).astype(BF16)

    if n_tp > 1:
        took(to.at[: n_tp - 1], t_r.at[0])
    middle_ref[:, xi] = heads_sum(xi)
    if n_in > 1:
        took(to.at[: (n_in - 1) * n_tp], t_r.at[3])
    for d in range(1, n_in):
        middle_ref[:, x_peer(d)] = heads_sum(x_peer(d))
    middle = middle_ref[...].reshape(batch, feats)

    def sum_groups(phase, buf, sem):
        for d in range(1, n_tp):
            launch(phase, buf.at[tp], buf.at[tp], sem, t_dev(d))
        if n_tp > 1:
            took(buf.at[: n_tp - 1], sem)
        total = buf[0].astype(F32)
        for g in range(1, n_tp):
            total = total + buf[g].astype(F32)
        return total

    load_mixer.wait()
    wide2 = middle.astype(F32)
    scaled2 = (wide2 * mixer_gain_ref[...].astype(F32).reshape(1, -1)).astype(BF16)
    took(wff, bulk_sem.at[2])
    d_order = list(range(n_c))
    if d_zf is not None:
        d_order = [0, d_zf] + list(range(1, d_zf))
    for k, c in enumerate(d_order):
        lo, hi = fbounds[c]
        scatter_rows(fx, jnp.dot(scaled2, wff[:, lo:hi], preferred_element_type=F32), lo)
        if c == d_zf:
            zf_send(1, fx, dfr, lo, hi)
        else:
            send_x(DX, fx, frx, fx_r.at[c], lo, hi)
        if k == min(SQ_AT, n_c - 1):
            squares_x(1, wide2)

    inv2 = [None]

    def to_z(c):
        lo, hi = fbounds[c]
        reduce_x(fx, frx, fz, fx_r.at[c], lo, hi)
        send_z(DZ, fz, frz, fz_r.at[c], lo, hi)
        if c == SQ_Z:
            squares_z(1)

    def activate(c):
        if c == d_zf:
            terms = zf_final(1, dfs, dfx)
        else:
            terms = reduce_z(fz, frz, fz_r.at[c], *fbounds[c])
        if inv2[0] is None:
            inv2[0] = inverse(1)
        terms = terms * inv2[0]
        fc = terms.shape[1] // 2
        cols = slice(*fchunks[c])
        hg[zi, xi, :, cols] = (jax.nn.silu(terms[:, :fc]) * terms[:, fc:]).astype(BF16)
        own = hg.at[zi, xi, :, cols]
        for d in range(1, n_out):
            launch(EZ, own, own, hz_r.at[c], z_dev(d))
        for d in range(1, n_in):
            launch(EX, own, own, hx_r.at[c], x_dev(d))

    def hand_on(c):
        cols = slice(*fchunks[c])
        if n_out > 1:
            took(hg.at[: n_out - 1, 0, :, cols], hz_r.at[c])
        for d in range(1, n_in):
            for z in range(1, n_out):
                slot = hg.at[z_back(z), xi, :, cols]
                launch(EX, slot, slot, hx_r.at[c], x_dev(d))

    steps = []
    for c in range(n_c):
        at = fchunks[c][1] / LANES
        if c == d_zf:
            steps.append((LAG_ZX, len(steps), lambda c: zf_to_x(1, fx, dfr, dfs, dfx, *fbounds[c]), c))
            steps.append((LAG_ZACT, len(steps), activate, c))
        else:
            steps.append((at, len(steps), to_z, c))
            steps.append((at + LAG_ACT, len(steps), activate, c))
        steps.append((at + LAG_HAND if c != d_zf else LAG_ZHAND, len(steps), hand_on, c))
    for _, _, step, c in sorted(steps, key=lambda item: item[:2]):
        step(c)

    load_dn.wait()
    down = None
    for c, (lo, hi) in enumerate(fchunks):
        if n_in > 1:
            took(hg.at[:, : n_in - 1, :, lo:hi], hx_r.at[c])
        term = jnp.dot(
            hg[:, :, :, lo:hi].reshape(batch, hi - lo),
            wdn[lo:hi, :],
            preferred_element_type=F32,
        )
        down = term if down is None else down + term
    td[tp] = down.astype(BF16)
    total = sum_groups(FY, td, t_r.at[1])
    wide3 = middle_ref[...].reshape(batch, feats).astype(F32)
    result_ref[...] = (wide3 + total).astype(BF16)

    def sent_but(ref, phase, ranges, but):
        left = sum(hi - lo for c, (lo, hi) in enumerate(ranges) if c != but)
        took(ref.at[..., :left], send_sem.at[phase])

    if a_zf is not None:
        took(zfr, send_sem.at[ZF])
        took(zfx, send_sem.at[XF])
    if d_zf is not None:
        took(dfr, send_sem.at[ZF + 1])
        took(dfx, send_sem.at[XF + 1])
    if n_in > 1:
        sent_but(rx, AX, bounds, a_zf)
        sent_but(frx, DX, fbounds, d_zf)
        took(wo.at[: n_in - 1], send_sem.at[BX])
        took(hg.at[:, : n_in - 1], send_sem.at[EX])
        for i in range(2):
            took(sqx.at[i, 1:n_in], send_sem.at[SQX + i])
    if n_out > 1:
        sent_but(rz, AZ, bounds, a_zf)
        sent_but(frz, DZ, fbounds, d_zf)
        took(mg.at[: n_out - 1], send_sem.at[BZ])
        took(hg.at[: n_out - 1, 0], send_sem.at[EZ])
        for i in range(2):
            took(sqz.at[i, 1:n_out], send_sem.at[SQZ + i])
    if n_in * n_tp > 1:
        took(to.at[: n_in * n_tp - 1], send_sem.at[CY])
    if n_tp > 1:
        took(td.at[: n_tp - 1], send_sem.at[FY])


def body(n_kv, n_tp, *args):
    (
        tokens,
        norm_gain,
        w_query,
        w_key,
        w_value,
        w_gate,
        w_decay,
        log_decay,
        state,
        out_gain,
        w_out,
        mixer_gain,
        w_ffgate,
        w_ffup,
        w_down,
    ) = args
    n_out, n_in = split_axis(n_kv)
    batch, feats = tokens.shape
    rows, heads, dk, dv = state.shape
    kw = w_query.shape[1]
    vw = w_value.shape[1]
    ff = w_ffgate.shape[1]
    n_in_out = n_in > 1 and n_out > 1
    fchunks = ff_chunks(ff, FF_Z if n_in_out else 0)
    n_c = len(fchunks)
    d_w = 2 * (fchunks[-1][1] - fchunks[-1][0])
    a_w = 2 * dk
    chunks, _, _, width = proj_layout(kw, vw, dk, dv)
    n_a = len(chunks)
    m_in, m_out = max(n_in - 1, 1), max(n_out - 1, 1)
    dma = pltpu.SemaphoreType.DMA
    vmem = pltpu.VMEM
    whole = pl.BlockSpec(memory_space=pltpu.VMEM)
    far = pl.BlockSpec(memory_space=pl.ANY)
    sems = [
        (3,),
        (n_a,),
        (4,),
        (PHASES,),
        (2, 2),
        (n_a,),
        (n_a,),
        (1,),
        (4,),
        (n_c,),
        (n_c,),
        (n_c,),
        (n_c,),
        (2, 2),
    ]
    result, new_state = pl.pallas_call(
        functools.partial(kernel, n_kv, n_tp, feats * n_kv),
        out_shape=(
            vmem((batch, feats), BF16),
            vmem(state.shape, F32),
        ),
        in_specs=[far] * 15,
        out_specs=(whole, whole),
        scratch_shapes=[
            vmem((batch, feats), BF16),
            vmem(norm_gain.shape, BF16),
            vmem(log_decay.shape, F32),
            vmem((1, dv), F32),
            vmem(mixer_gain.shape, BF16),
            vmem((feats, width), BF16),
            vmem((n_in,) + w_out.shape, BF16),
            vmem((feats, 2 * ff), BF16),
            vmem(w_down.shape, BF16),
            vmem((2, n_in, SUBLANES, batch), F32),
            vmem((2, n_out, SUBLANES, batch), F32),
            vmem((n_in, n_out, rows, width), BF16),
            vmem((m_in, n_out, rows, width), BF16),
            vmem((n_out, rows, width), BF16),
            vmem((m_out, rows, width), BF16),
            vmem((heads, rows, dv), F32),
            vmem((n_out, rows, vw), BF16),
            vmem((n_in * n_tp, n_out * rows, feats), BF16),
            vmem((m_in, n_out * rows, feats), BF16),
            vmem((n_in, n_out, rows, 2 * ff), BF16),
            vmem((m_in, n_out, rows, 2 * ff), BF16),
            vmem((n_out, rows, 2 * ff), BF16),
            vmem((m_out, rows, 2 * ff), BF16),
            vmem((n_out, n_in, rows, ff), BF16),
            vmem((n_tp, batch, feats), BF16),
            vmem((n_out, n_in, rows, feats), BF16),
            vmem((m_out, n_in, rows, a_w), BF16),
            vmem((n_in, rows, a_w), BF16),
            vmem((m_in, rows, a_w), BF16),
            vmem((m_out, n_in, rows, d_w), BF16),
            vmem((n_in, rows, d_w), BF16),
            vmem((m_in, rows, d_w), BF16),
        ]
        + [dma(shape) for shape in sems],
        compiler_params=pltpu.CompilerParams(
            collective_id=0, has_side_effects=True, vmem_limit_bytes=56 * 2**20
        ),
    )(
        tokens,
        norm_gain,
        w_query,
        w_key,
        w_value,
        w_gate,
        w_decay,
        log_decay,
        state,
        out_gain.reshape(1, dv),
        w_out,
        mixer_gain,
        w_ffgate,
        w_ffup,
        w_down,
    )
    return (result, new_state)


def solution(mesh):
    return jax.shard_map(
        functools.partial(body, mesh.shape["kv"], mesh.shape["tp"]),
        mesh=mesh,
        in_specs=(
            P(None, "kv"),
            P("kv"),
            P("kv", "tp"),
            P("kv", "tp"),
            P("kv", "tp"),
            P("kv", "tp"),
            P("kv", "tp"),
            P("kv", "tp"),
            P("kv", "tp", None, None),
            P(),
            P("tp", "kv"),
            P("kv"),
            P("kv", "tp"),
            P("kv", "tp"),
            P("tp", "kv"),
        ),
        out_specs=(P(None, "kv"), P("kv", "tp", None, None)),
        check_vma=False,
    )
```

```python
import functools

import jax
import jax.numpy as jnp
from jax import lax
from jax.experimental import pallas as pl
from jax.experimental.pallas import tpu as pltpu
from jax.sharding import PartitionSpec as P

eps = 1e-06
gate_norm = 16.0
LANES = 128
SUBLANES = 8
FF_SIZES = (1,)
FF_Z = 2
FAR_FIRST = 1
LAG_ZX = 8
SQ_AT = 1
A_SQ = 0
A_SQZ = 0
SQ_Z = 0
A_ZF = 1
LAG_ZACT = 12
LAG_ACT = 11
LAG_HAND = 100
LAG_ZHAND = 100
AX, AZ, BZ, BX, CY, DX, DZ, EZ, EX, FY, SQX, SQZ, ZF, XF, PHASES = 0, 1, 2, 3, 4, 5, 6, 7, 8, 9, 10, 12, 14, 16, 18
F32 = jnp.float32
BF16 = jnp.bfloat16


def remote(src, dst, send_sem, recv_sem, device):
    return pltpu.make_async_remote_copy(
        src_ref=src,
        dst_ref=dst,
        send_sem=send_sem,
        recv_sem=recv_sem,
        device_id=device,
        device_id_type=pl.DeviceIdType.MESH,
    )


def split_axis(n_kv):
    n_in = 1
    while n_in * n_in * 4 <= n_kv:
        n_in *= 2
    return n_kv // n_in, n_in


def ff_chunks(width, z_units):
    if width % LANES:
        return [(0, width)]
    units = width // LANES
    tail = z_units if z_units < units else 0
    left, sizes, k = units - tail, [], 0
    while left:
        take = min(left, FF_SIZES[min(k, len(FF_SIZES) - 1)])
        sizes.append(take)
        left -= take
        k += 1
    if tail:
        sizes.append(tail)
    at, ranges = 0, []
    for take in sizes:
        ranges.append((at, at + take * LANES))
        at += take * LANES
    return ranges


def proj_layout(kw, vw, dk, dv):
    heads = kw // dk
    at, chunks, where = 0, [], []

    def put(items):
        nonlocal at
        pieces, places = [], []
        for weight, lo, width in items:
            pieces.append((weight, lo, width, at))
            places.append(at)
            at += width
        chunks.append(pieces)
        return places

    for h in range(heads):
        q, k = put([("q", h * dk, dk), ("k", h * dk, dk)])
        d, v = put([("d", h * dk, dk), ("v", h * dv, dv)])
        where.append((q, k, d, v))
    (g,) = put([("g", 0, vw)])
    return chunks, where, g, at


def kernel(
    n_kv,
    n_tp,
    d_model,
    tokens_hbm,
    norm_gain_hbm,
    wq_hbm,
    wk_hbm,
    wv_hbm,
    wg_hbm,
    wd_hbm,
    log_decay_hbm,
    state_hbm,
    out_gain_hbm,
    wo_hbm,
    mixer_gain_hbm,
    wfg_hbm,
    wfu_hbm,
    wdn_hbm,
    result_ref,
    ns_ref,
    tokens_ref,
    norm_gain_ref,
    log_decay_ref,
    out_gain_ref,
    mixer_gain_ref,
    wall,
    wo,
    wff,
    wdn,
    sqx,
    sqz,
    px,
    rx,
    pz,
    rz,
    att,
    mg,
    to,
    away,
    fx,
    frx,
    fz,
    frz,
    hg,
    td,
    middle_ref,
    zfr,
    zfs,
    zfx,
    dfr,
    dfs,
    dfx,
    in_sem,
    w_sem,
    bulk_sem,
    send_sem,
    sq_r,
    mz_r,
    t_r,
    fx_r,
    fz_r,
    hx_r,
    zf_r,
):
    n_out, n_in = split_axis(n_kv)
    kv = lax.axis_index("kv")
    tp = lax.axis_index("tp")
    zi = kv // n_in
    xi = lax.rem(kv, n_in)
    rows = px.shape[2]
    batch, feats = tokens_ref.shape
    heads, dk, dv = ns_ref.shape[1:]
    kw = wq_hbm.shape[1]
    vw = wv_hbm.shape[1]
    ff = wfg_hbm.shape[1]

    def x_peer(d):
        return lax.rem(xi + d, n_in)

    def z_peer(d):
        return lax.rem(zi + d, n_out)

    def z_back(d):
        return lax.rem(zi + n_out - d, n_out)

    def x_dev(d):
        return (zi * n_in + x_peer(d), tp)

    def z_dev(d):
        return (z_peer(d) * n_in + xi, tp)

    def t_dev(d):
        return (kv, lax.rem(tp + d, n_tp))

    def z_targets():
        if n_out % 2 or not FAR_FIRST:
            return [(z_peer(d), d) for d in range(1, n_out)]
        up = zi // (n_out // 2)
        found = []
        for j in range(n_out - 1):
            high = n_out - 1 - j
            from_top = high - 1 + (high - zi + n_out - 1) // n_out
            from_bottom = j + 1 - (zi - j + n_out - 1) // n_out
            target = up * from_bottom + (1 - up) * from_top
            found.append((target, lax.rem(target - zi + n_out, n_out)))
        return found

    z_order = z_targets()

    def xt_dev(d, e):
        return (zi * n_in + x_peer(d), lax.rem(tp + e, n_tp))

    barrier = pltpu.get_barrier_semaphore()
    peers = [z_dev(d) for d in range(1, n_out)] + [
        xt_dev(d, e) for d in range(n_in) for e in range(n_tp) if d or e
    ]
    for dev in peers:
        pl.semaphore_signal(barrier, inc=1, device_id=dev, device_id_type=pl.DeviceIdType.MESH)

    def fetch(src, dst, sem):
        copy = pltpu.make_async_copy(src, dst, sem)
        copy.start()
        return copy

    chunks, where, g_at, width = proj_layout(kw, vw, dk, dv)
    source = {"q": wq_hbm, "k": wk_hbm, "d": wd_hbm, "v": wv_hbm, "g": wg_hbm}
    first_loads = [
        fetch(tokens_hbm, tokens_ref, in_sem.at[0]),
        fetch(norm_gain_hbm, norm_gain_ref, in_sem.at[1]),
    ]
    bounds = []
    two_way = n_in > 1 and n_out > 1
    a_zf = 2 * (heads - 1) if two_way and A_ZF else None
    order = [0] + sorted(range(1, len(chunks)), key=lambda c: (c != a_zf, c))
    for c in order:
        for name, lo, wide, at in chunks[c]:
            fetch(source[name].at[:, lo : lo + wide], wall.at[:, at : at + wide], w_sem.at[c])
    for pieces in chunks:
        bounds.append((pieces[0][3], pieces[-1][3] + pieces[-1][2]))

    def took(ref, sem):
        pltpu.make_async_copy(ref, ref, sem).wait()

    def launch(phase, src, dst, recv_sem, device):
        remote(src, dst, send_sem.at[phase], recv_sem, device).start()

    def scatter_rows(dst, value, lo):
        wide = value.shape[1]
        value = value.astype(BF16)
        for z in range(n_out):
            for x in range(n_in):
                at = (z * n_in + x) * rows
                dst[x, z, :, lo : lo + wide] = value[at : at + rows]

    def send_x(phase, src, dst, sem, lo, hi):
        for d in range(1, n_in):
            launch(
                phase,
                src.at[x_peer(d), :, :, lo:hi],
                dst.at[d - 1, :, :, lo:hi],
                sem,
                x_dev(d),
            )

    def send_z(phase, src, dst, sem, lo, hi):
        for z, d in z_order:
            launch(
                phase,
                src.at[z, :, lo:hi],
                dst.at[d - 1, :, lo:hi],
                sem,
                (z * n_in + xi, tp),
            )

    def reduce_x(src, got, dst, sem, lo, hi):
        total = src[xi, :, :, lo:hi].astype(F32)
        if n_in > 1:
            took(got.at[:, :, :, lo:hi], sem)
            for d in range(1, n_in):
                total = total + got[d - 1, :, :, lo:hi].astype(F32)
        dst[:, :, lo:hi] = total.astype(BF16)

    def reduce_z(src, got, sem, lo, hi):
        total = src[zi, :, lo:hi].astype(F32)
        if n_out > 1:
            took(got.at[:, :, lo:hi], sem)
            for d in range(1, n_out):
                total = total + got[d - 1, :, lo:hi].astype(F32)
        return total

    def zf_send(i, src, dst, lo, hi):
        for z, d in z_order:
            launch(ZF + i, src.at[:, z, :, lo:hi], dst.at[d - 1], zf_r.at[i, 0], (z * n_in + xi, tp))

    def zf_to_x(i, src, got, mid, dst, lo, hi):
        took(got, zf_r.at[i, 0])
        total = src[:, zi, :, lo:hi].astype(F32)
        for d in range(1, n_out):
            total = total + got[d - 1].astype(F32)
        mid[...] = total.astype(BF16)
        for d in range(1, n_in):
            launch(XF + i, mid.at[x_peer(d)], dst.at[d - 1], zf_r.at[i, 1], x_dev(d))

    def zf_final(i, mid, got):
        took(got, zf_r.at[i, 1])
        total = mid[xi].astype(F32)
        for d in range(1, n_in):
            total = total + got[d - 1].astype(F32)
        return total

    def squares_x(i, values):
        ones = jnp.ones((SUBLANES, feats), F32)
        sqx[i, 0] = lax.dot_general(
            ones,
            values * values,
            (((1,), (1,)), ((), ())),
            precision=lax.Precision.HIGHEST,
            preferred_element_type=F32,
        )
        for d in range(1, n_in):
            launch(SQX + i, sqx.at[i, 0], sqx.at[i, d], sq_r.at[i, 0], x_dev(d))

    def squares_z(i):
        if n_in > 1:
            took(sqx.at[i, 1:n_in], sq_r.at[i, 0])
        total = sqx[i, 0]
        for d in range(1, n_in):
            total = total + sqx[i, d]
        sqz[i, 0] = total
        for z, d in z_order:
            launch(SQZ + i, sqz.at[i, 0], sqz.at[i, d], sq_r.at[i, 1], (z * n_in + xi, tp))

    def inverse(i):
        if n_out > 1:
            took(sqz.at[i, 1:n_out], sq_r.at[i, 1])
        total = sqz[i, 0]
        for d in range(1, n_out):
            total = total + sqz[i, d]
        lane = lax.broadcasted_iota(jnp.int32, (rows, batch), 1)
        mine = lax.broadcasted_iota(jnp.int32, (rows, batch), 0) + kv * rows
        own = jnp.where(lane == mine, jnp.broadcast_to(total[:1], (rows, batch)), 0.0)
        return lax.rsqrt(jnp.sum(own, axis=1, keepdims=True) / d_model + eps)

    for load in first_loads:
        load.wait()
    wide = tokens_ref[...].astype(F32)
    scaled = (wide * norm_gain_ref[...].astype(F32).reshape(1, -1)).astype(BF16)

    for k, c in enumerate(order):
        lo, hi = bounds[c]
        took(wall.at[:, lo:hi], w_sem.at[c])
        scatter_rows(px, jnp.dot(scaled, wall[:, lo:hi], preferred_element_type=F32), lo)
        if k == 0:
            pl.semaphore_wait(barrier, len(peers))
        if c == a_zf:
            zf_send(0, px, zfr, lo, hi)
        else:
            send_x(AX, px, rx, fx_r.at[c], lo, hi)
        if k == A_SQ:
            squares_x(0, wide)
    load_decay = fetch(log_decay_hbm, log_decay_ref, in_sem.at[0])
    load_gain = fetch(out_gain_hbm, out_gain_ref, in_sem.at[1])
    load_mixer = fetch(mixer_gain_hbm, mixer_gain_ref, in_sem.at[2])
    load_state = fetch(state_hbm, ns_ref, bulk_sem.at[0])
    load_o = fetch(wo_hbm, wo.at[xi], bulk_sem.at[1])
    fchunks = ff_chunks(ff, FF_Z if two_way else 0)
    n_c = len(fchunks)
    d_zf = n_c - 1 if two_way and n_c > 1 else None
    fbounds = [(2 * lo, 2 * hi) for lo, hi in fchunks]
    for lo, hi in fchunks:
        fetch(wfg_hbm.at[:, lo:hi], wff.at[:, 2 * lo : lo + hi], bulk_sem.at[2])
        fetch(wfu_hbm.at[:, lo:hi], wff.at[:, lo + hi : 2 * hi], bulk_sem.at[2])
    load_dn = fetch(wdn_hbm, wdn, bulk_sem.at[3])

    x_order = [c for c in order if c != a_zf]
    for k, c in enumerate(x_order):
        lo, hi = bounds[c]
        if a_zf is not None and k == len(x_order) - 1:
            zf_to_x(0, px, zfr, zfs, zfx, *bounds[a_zf])
        reduce_x(px, rx, pz, fx_r.at[c], lo, hi)
        send_z(AZ, pz, rz, fz_r.at[c], lo, hi)
        if k == A_SQZ:
            squares_z(0)

    for d in range(1, n_in):
        launch(BX, wo_hbm, wo.at[xi], t_r.at[2], x_dev(d))

    def arrived(c):
        if c == a_zf:
            return zf_final(0, zfs, zfx)
        return reduce_z(pz, rz, fz_r.at[c], *bounds[c])


    load_decay.wait()
    load_state.wait()
    inv = None
    for h in range(heads):
        c = 2 * h
        q_at, k_at, d_at, v_at = (at for at in where[h])
        qk = arrived(c)
        if h == 0:
            inv = inverse(0)
        qk = qk * inv
        dv_terms = arrived(c + 1) * inv
        query = qk[:, :dk] * dk ** (-0.5)
        pre = dv_terms[:, :dk]
        values = dv_terms[:, dk:]
        log_sig = jnp.minimum(pre, 0.0) - jnp.log1p(jnp.exp(-jnp.abs(pre)))
        decay = jnp.exp(log_sig / gate_norm + log_decay_ref[:, h * dk : (h + 1) * dk])
        q_t = query.T
        k_t = qk[:, dk:].T
        a_t = decay.T
        for b in range(rows):
            col = slice(b, b + 1)
            new = ns_ref[b, h] * a_t[:, col] + k_t[:, col] * values[col, :]
            ns_ref[b, h] = new
            att[h, col, :] = jnp.sum(new * q_t[:, col], axis=0, keepdims=True)

    load_gain.wait()
    last = len(bounds) - 1
    gate = reduce_z(pz, rz, fz_r.at[last], *bounds[last]) * inv
    for h in range(heads):
        got = att[h]
        normed = (
            got
            * lax.rsqrt(jnp.mean(got * got, axis=1, keepdims=True) + eps)
            * out_gain_ref[...]
        )
        cols = slice(h * dv, (h + 1) * dv)
        mg[zi, :, cols] = (normed * jax.nn.silu(gate[:, cols])).astype(BF16)

    own = mg.at[zi]
    for z, _ in z_order:
        launch(BZ, own, own, mz_r.at[0], (z * n_in + xi, tp))
    load_o.wait()
    if n_in > 1:
        took(wo.at[: n_in - 1], t_r.at[2])
    if n_out > 1:
        took(mg.at[: n_out - 1], mz_r.at[0])
    mixed = mg[...].reshape(n_out * rows, vw)
    mine = xi * n_tp + tp
    for d in range(1, n_in):
        part = jnp.dot(mixed, wo[x_peer(d)], preferred_element_type=F32)
        away[d - 1] = part.astype(BF16)
        for e in range(n_tp):
            launch(CY, away.at[d - 1], to.at[mine], t_r.at[3], xt_dev(d, e))
    to[mine] = jnp.dot(mixed, wo[xi], preferred_element_type=F32).astype(BF16)
    for e in range(1, n_tp):
        launch(CY, to.at[mine], to.at[mine], t_r.at[0], t_dev(e))

    def heads_sum(x):
        total = to[x * n_tp].astype(F32)
        for g in range(1, n_tp):
            total = total + to[x * n_tp + g].astype(F32)
        tok = jnp.stack(
            [tokens_ref[pl.ds((z * n_in + x) * rows, rows), :] for z in range(n_out)]
        )
        return (tok.astype(F32) + total.reshape(n_out, rows, feats)).astype(BF16)

    if n_tp > 1:
        took(to.at[: n_tp - 1], t_r.at[0])
    middle_ref[:, xi] = heads_sum(xi)
    if n_in > 1:
        took(to.at[: (n_in - 1) * n_tp], t_r.at[3])
    for d in range(1, n_in):
        middle_ref[:, x_peer(d)] = heads_sum(x_peer(d))
    middle = middle_ref[...].reshape(batch, feats)

    def sum_groups(phase, buf, sem):
        for d in range(1, n_tp):
            launch(phase, buf.at[tp], buf.at[tp], sem, t_dev(d))
        if n_tp > 1:
            took(buf.at[: n_tp - 1], sem)
        total = buf[0].astype(F32)
        for g in range(1, n_tp):
            total = total + buf[g].astype(F32)
        return total

    load_mixer.wait()
    wide2 = middle.astype(F32)
    scaled2 = (wide2 * mixer_gain_ref[...].astype(F32).reshape(1, -1)).astype(BF16)
    took(wff, bulk_sem.at[2])
    d_order = list(range(n_c))
    if d_zf is not None:
        d_order = [0, d_zf] + list(range(1, d_zf))
    for k, c in enumerate(d_order):
        lo, hi = fbounds[c]
        scatter_rows(fx, jnp.dot(scaled2, wff[:, lo:hi], preferred_element_type=F32), lo)
        if c == d_zf:
            zf_send(1, fx, dfr, lo, hi)
        else:
            send_x(DX, fx, frx, fx_r.at[c], lo, hi)
        if k == min(SQ_AT, n_c - 1):
            squares_x(1, wide2)

    inv2 = [None]

    def to_z(c):
        lo, hi = fbounds[c]
        reduce_x(fx, frx, fz, fx_r.at[c], lo, hi)
        send_z(DZ, fz, frz, fz_r.at[c], lo, hi)
        if c == SQ_Z:
            squares_z(1)

    def activate(c):
        if c == d_zf:
            terms = zf_final(1, dfs, dfx)
        else:
            terms = reduce_z(fz, frz, fz_r.at[c], *fbounds[c])
        if inv2[0] is None:
            inv2[0] = inverse(1)
        terms = terms * inv2[0]
        fc = terms.shape[1] // 2
        cols = slice(*fchunks[c])
        hg[zi, xi, :, cols] = (jax.nn.silu(terms[:, :fc]) * terms[:, fc:]).astype(BF16)
        own = hg.at[zi, xi, :, cols]
        for z, _ in z_order:
            launch(EZ, own, own, fx_r.at[c], (z * n_in + xi, tp))
        for d in range(1, n_in):
            launch(EX, own, own, hx_r.at[c], x_dev(d))

    def hand_on(c):
        cols = slice(*fchunks[c])
        if n_out > 1:
            took(hg.at[: n_out - 1, 0, :, cols], fx_r.at[c])
        for d in range(1, n_in):
            for z in range(1, n_out):
                slot = hg.at[z_back(z), xi, :, cols]
                launch(EX, slot, slot, hx_r.at[c], x_dev(d))

    steps = []
    for c in range(n_c):
        at = fchunks[c][1] / LANES
        if c == d_zf:
            steps.append((LAG_ZX, len(steps), lambda c: zf_to_x(1, fx, dfr, dfs, dfx, *fbounds[c]), c))
            steps.append((LAG_ZACT, len(steps), activate, c))
        else:
            steps.append((at, len(steps), to_z, c))
            steps.append((at + LAG_ACT, len(steps), activate, c))
        steps.append((at + LAG_HAND if c != d_zf else LAG_ZHAND, len(steps), hand_on, c))
    for _, _, step, c in sorted(steps, key=lambda item: item[:2]):
        step(c)

    load_dn.wait()
    down = None
    for c, (lo, hi) in enumerate(fchunks):
        if n_in > 1:
            took(hg.at[:, : n_in - 1, :, lo:hi], hx_r.at[c])
        term = jnp.dot(
            hg[:, :, :, lo:hi].reshape(batch, hi - lo),
            wdn[lo:hi, :],
            preferred_element_type=F32,
        )
        down = term if down is None else down + term
    td[tp] = down.astype(BF16)
    total = sum_groups(FY, td, t_r.at[1])
    wide3 = middle_ref[...].reshape(batch, feats).astype(F32)
    result_ref[...] = (wide3 + total).astype(BF16)

    def sent_but(ref, phase, ranges, but):
        left = sum(hi - lo for c, (lo, hi) in enumerate(ranges) if c != but)
        took(ref.at[..., :left], send_sem.at[phase])

    if a_zf is not None:
        took(zfr, send_sem.at[ZF])
        took(zfx, send_sem.at[XF])
    if d_zf is not None:
        took(dfr, send_sem.at[ZF + 1])
        took(dfx, send_sem.at[XF + 1])
    if n_in > 1:
        sent_but(rx, AX, bounds, a_zf)
        sent_but(frx, DX, fbounds, d_zf)
        took(wo.at[: n_in - 1], send_sem.at[BX])
        took(hg.at[:, : n_in - 1], send_sem.at[EX])
        for i in range(2):
            took(sqx.at[i, 1:n_in], send_sem.at[SQX + i])
    if n_out > 1:
        sent_but(rz, AZ, bounds, a_zf)
        sent_but(frz, DZ, fbounds, d_zf)
        took(mg.at[: n_out - 1], send_sem.at[BZ])
        took(hg.at[: n_out - 1, 0], send_sem.at[EZ])
        for i in range(2):
            took(sqz.at[i, 1:n_out], send_sem.at[SQZ + i])
    if n_in * n_tp > 1:
        took(to.at[: n_in * n_tp - 1], send_sem.at[CY])
    if n_tp > 1:
        took(td.at[: n_tp - 1], send_sem.at[FY])


def body(n_kv, n_tp, *args):
    (
        tokens,
        norm_gain,
        w_query,
        w_key,
        w_value,
        w_gate,
        w_decay,
        log_decay,
        state,
        out_gain,
        w_out,
        mixer_gain,
        w_ffgate,
        w_ffup,
        w_down,
    ) = args
    n_out, n_in = split_axis(n_kv)
    batch, feats = tokens.shape
    rows, heads, dk, dv = state.shape
    kw = w_query.shape[1]
    vw = w_value.shape[1]
    ff = w_ffgate.shape[1]
    n_in_out = n_in > 1 and n_out > 1
    fchunks = ff_chunks(ff, FF_Z if n_in_out else 0)
    n_c = len(fchunks)
    d_w = 2 * (fchunks[-1][1] - fchunks[-1][0])
    a_w = 2 * dk
    chunks, _, _, width = proj_layout(kw, vw, dk, dv)
    n_a = len(chunks)
    m_in, m_out = max(n_in - 1, 1), max(n_out - 1, 1)
    dma = pltpu.SemaphoreType.DMA
    vmem = pltpu.VMEM
    whole = pl.BlockSpec(memory_space=pltpu.VMEM)
    far = pl.BlockSpec(memory_space=pl.ANY)
    sems = [
        (3,),
        (n_a,),
        (4,),
        (PHASES,),
        (2, 2),
        (1,),
        (4,),
        (max(n_a, n_c),),
        (max(n_a, n_c),),
        (n_c,),
        (2, 2),
    ]
    result, new_state = pl.pallas_call(
        functools.partial(kernel, n_kv, n_tp, feats * n_kv),
        out_shape=(
            vmem((batch, feats), BF16),
            vmem(state.shape, F32),
        ),
        in_specs=[far] * 15,
        out_specs=(whole, whole),
        scratch_shapes=[
            vmem((batch, feats), BF16),
            vmem(norm_gain.shape, BF16),
            vmem(log_decay.shape, F32),
            vmem((1, dv), F32),
            vmem(mixer_gain.shape, BF16),
            vmem((feats, width), BF16),
            vmem((n_in,) + w_out.shape, BF16),
            vmem((feats, 2 * ff), BF16),
            vmem(w_down.shape, BF16),
            vmem((2, n_in, SUBLANES, batch), F32),
            vmem((2, n_out, SUBLANES, batch), F32),
            vmem((n_in, n_out, rows, width), BF16),
            vmem((m_in, n_out, rows, width), BF16),
            vmem((n_out, rows, width), BF16),
            vmem((m_out, rows, width), BF16),
            vmem((heads, rows, dv), F32),
            vmem((n_out, rows, vw), BF16),
            vmem((n_in * n_tp, n_out * rows, feats), BF16),
            vmem((m_in, n_out * rows, feats), BF16),
            vmem((n_in, n_out, rows, 2 * ff), BF16),
            vmem((m_in, n_out, rows, 2 * ff), BF16),
            vmem((n_out, rows, 2 * ff), BF16),
            vmem((m_out, rows, 2 * ff), BF16),
            vmem((n_out, n_in, rows, ff), BF16),
            vmem((n_tp, batch, feats), BF16),
            vmem((n_out, n_in, rows, feats), BF16),
            vmem((m_out, n_in, rows, a_w), BF16),
            vmem((n_in, rows, a_w), BF16),
            vmem((m_in, rows, a_w), BF16),
            vmem((m_out, n_in, rows, d_w), BF16),
            vmem((n_in, rows, d_w), BF16),
            vmem((m_in, rows, d_w), BF16),
        ]
        + [dma(shape) for shape in sems],
        compiler_params=pltpu.CompilerParams(
            collective_id=0, has_side_effects=True, vmem_limit_bytes=56 * 2**20
        ),
    )(
        tokens,
        norm_gain,
        w_query,
        w_key,
        w_value,
        w_gate,
        w_decay,
        log_decay,
        state,
        out_gain.reshape(1, dv),
        w_out,
        mixer_gain,
        w_ffgate,
        w_ffup,
        w_down,
    )
    return (result, new_state)


def solution(mesh):
    return jax.shard_map(
        functools.partial(body, mesh.shape["kv"], mesh.shape["tp"]),
        mesh=mesh,
        in_specs=(
            P(None, "kv"),
            P("kv"),
            P("kv", "tp"),
            P("kv", "tp"),
            P("kv", "tp"),
            P("kv", "tp"),
            P("kv", "tp"),
            P("kv", "tp"),
            P("kv", "tp", None, None),
            P(),
            P("tp", "kv"),
            P("kv"),
            P("kv", "tp"),
            P("kv", "tp"),
            P("tp", "kv"),
        ),
        out_specs=(P(None, "kv"), P("kv", "tp", None, None)),
        check_vma=False,
    )
```

```python
import functools

import jax
import jax.numpy as jnp
from jax import lax
from jax.experimental import pallas as pl
from jax.experimental.pallas import tpu as pltpu
from jax.sharding import PartitionSpec as P

eps = 1e-06
gate_norm = 16.0
LANES = 128
SUBLANES = 8
FF_SIZES = (1,)
FF_Z = 2
FAR_FIRST = 1
DIRECT = 2
LAG_ZX = 8
SQ_AT = 1
A_SQ = 0
A_SQZ = 0
SQ_Z = 0
A_ZF = 1
LAG_ZACT = 12
LAG_ACT = 11
LAG_HAND = 100
LAG_ZHAND = 100
AX, AZ, BZ, BX, CY, DX, DZ, EZ, EX, FY, SQX, SQZ, ZF, XF, PHASES = 0, 1, 2, 3, 4, 5, 6, 7, 8, 9, 10, 12, 14, 16, 18
F32 = jnp.float32
BF16 = jnp.bfloat16


def remote(src, dst, send_sem, recv_sem, device):
    return pltpu.make_async_remote_copy(
        src_ref=src,
        dst_ref=dst,
        send_sem=send_sem,
        recv_sem=recv_sem,
        device_id=device,
        device_id_type=pl.DeviceIdType.MESH,
    )


def split_axis(n_kv):
    n_in = 1
    while n_in * n_in * 4 <= n_kv:
        n_in *= 2
    return n_kv // n_in, n_in


def ff_chunks(width, z_units):
    if width % LANES:
        return [(0, width)]
    units = width // LANES
    tail = z_units if z_units < units else 0
    left, sizes, k = units - tail, [], 0
    while left:
        take = min(left, FF_SIZES[min(k, len(FF_SIZES) - 1)])
        sizes.append(take)
        left -= take
        k += 1
    if tail:
        sizes.append(tail)
    at, ranges = 0, []
    for take in sizes:
        ranges.append((at, at + take * LANES))
        at += take * LANES
    return ranges


def proj_layout(kw, vw, dk, dv):
    heads = kw // dk
    at, chunks, where = 0, [], []

    def put(items):
        nonlocal at
        pieces, places = [], []
        for weight, lo, width in items:
            pieces.append((weight, lo, width, at))
            places.append(at)
            at += width
        chunks.append(pieces)
        return places

    for h in range(heads):
        q, k = put([("q", h * dk, dk), ("k", h * dk, dk)])
        d, v = put([("d", h * dk, dk), ("v", h * dv, dv)])
        where.append((q, k, d, v))
    (g,) = put([("g", 0, vw)])
    return chunks, where, g, at


def kernel(
    n_kv,
    n_tp,
    d_model,
    tokens_hbm,
    norm_gain_hbm,
    wq_hbm,
    wk_hbm,
    wv_hbm,
    wg_hbm,
    wd_hbm,
    log_decay_hbm,
    state_hbm,
    out_gain_hbm,
    wo_hbm,
    mixer_gain_hbm,
    wfg_hbm,
    wfu_hbm,
    wdn_hbm,
    result_ref,
    ns_ref,
    tokens_ref,
    norm_gain_ref,
    log_decay_ref,
    out_gain_ref,
    mixer_gain_ref,
    wall,
    wo,
    wff,
    wdn,
    sqx,
    sqz,
    px,
    rx,
    pz,
    rz,
    att,
    mg,
    to,
    away,
    fx,
    frx,
    fz,
    frz,
    hg,
    td,
    middle_ref,
    zfr,
    zfs,
    zfx,
    dfr,
    dfs,
    dfx,
    in_sem,
    w_sem,
    bulk_sem,
    send_sem,
    sq_r,
    mz_r,
    t_r,
    fx_r,
    fz_r,
    hx_r,
    zf_r,
):
    n_out, n_in = split_axis(n_kv)
    kv = lax.axis_index("kv")
    tp = lax.axis_index("tp")
    zi = kv // n_in
    xi = lax.rem(kv, n_in)
    rows = px.shape[2]
    batch, feats = tokens_ref.shape
    heads, dk, dv = ns_ref.shape[1:]
    kw = wq_hbm.shape[1]
    vw = wv_hbm.shape[1]
    ff = wfg_hbm.shape[1]

    def x_peer(d):
        return lax.rem(xi + d, n_in)

    def z_peer(d):
        return lax.rem(zi + d, n_out)

    def z_back(d):
        return lax.rem(zi + n_out - d, n_out)

    def x_dev(d):
        return (zi * n_in + x_peer(d), tp)

    def z_dev(d):
        return (z_peer(d) * n_in + xi, tp)

    def t_dev(d):
        return (kv, lax.rem(tp + d, n_tp))

    def z_targets():
        if n_out % 2 or not FAR_FIRST:
            return [(z_peer(d), d) for d in range(1, n_out)]
        up = zi // (n_out // 2)
        found = []
        for j in range(n_out - 1):
            high = n_out - 1 - j
            from_top = high - 1 + (high - zi + n_out - 1) // n_out
            from_bottom = j + 1 - (zi - j + n_out - 1) // n_out
            target = up * from_bottom + (1 - up) * from_top
            found.append((target, lax.rem(target - zi + n_out, n_out)))
        return found

    z_order = z_targets()

    def xt_dev(d, e):
        return (zi * n_in + x_peer(d), lax.rem(tp + e, n_tp))

    barrier = pltpu.get_barrier_semaphore()
    peers = [z_dev(d) for d in range(1, n_out)] + [
        xt_dev(d, e) for d in range(n_in) for e in range(n_tp) if d or e
    ]
    for dev in peers:
        pl.semaphore_signal(barrier, inc=1, device_id=dev, device_id_type=pl.DeviceIdType.MESH)

    def fetch(src, dst, sem):
        copy = pltpu.make_async_copy(src, dst, sem)
        copy.start()
        return copy

    chunks, where, g_at, width = proj_layout(kw, vw, dk, dv)
    source = {"q": wq_hbm, "k": wk_hbm, "d": wd_hbm, "v": wv_hbm, "g": wg_hbm}
    first_loads = [
        fetch(tokens_hbm, tokens_ref, in_sem.at[0]),
        fetch(norm_gain_hbm, norm_gain_ref, in_sem.at[1]),
    ]
    bounds = []
    two_way = n_in > 1 and n_out > 1
    a_zf = 2 * (heads - 1) if two_way and A_ZF else None
    order = [0] + sorted(range(1, len(chunks)), key=lambda c: (c != a_zf, c))
    for c in order:
        for name, lo, wide, at in chunks[c]:
            fetch(source[name].at[:, lo : lo + wide], wall.at[:, at : at + wide], w_sem.at[c])
    for pieces in chunks:
        bounds.append((pieces[0][3], pieces[-1][3] + pieces[-1][2]))

    def took(ref, sem):
        pltpu.make_async_copy(ref, ref, sem).wait()

    def launch(phase, src, dst, recv_sem, device):
        remote(src, dst, send_sem.at[phase], recv_sem, device).start()

    def scatter_rows(dst, value, lo):
        wide = value.shape[1]
        value = value.astype(BF16)
        for z in range(n_out):
            for x in range(n_in):
                at = (z * n_in + x) * rows
                dst[x, z, :, lo : lo + wide] = value[at : at + rows]

    def send_x(phase, src, dst, sem, lo, hi):
        for d in range(1, n_in):
            launch(
                phase,
                src.at[x_peer(d), :, :, lo:hi],
                dst.at[d - 1, :, :, lo:hi],
                sem,
                x_dev(d),
            )

    def send_z(phase, src, dst, sem, lo, hi):
        for z, d in z_order:
            launch(
                phase,
                src.at[z, :, lo:hi],
                dst.at[d - 1, :, lo:hi],
                sem,
                (z * n_in + xi, tp),
            )

    def reduce_x(src, got, dst, sem, lo, hi):
        total = src[xi, :, :, lo:hi].astype(F32)
        if n_in > 1:
            took(got.at[:, :, :, lo:hi], sem)
            for d in range(1, n_in):
                total = total + got[d - 1, :, :, lo:hi].astype(F32)
        dst[:, :, lo:hi] = total.astype(BF16)

    def reduce_z(src, got, sem, lo, hi):
        total = src[zi, :, lo:hi].astype(F32)
        if n_out > 1:
            took(got.at[:, :, lo:hi], sem)
            for d in range(1, n_out):
                total = total + got[d - 1, :, lo:hi].astype(F32)
        return total

    def zf_send(i, src, dst, lo, hi):
        for z, d in z_order:
            launch(ZF + i, src.at[:, z, :, lo:hi], dst.at[d - 1], zf_r.at[i, 0], (z * n_in + xi, tp))

    def zf_to_x(i, src, got, mid, dst, lo, hi):
        took(got, zf_r.at[i, 0])
        total = src[:, zi, :, lo:hi].astype(F32)
        for d in range(1, n_out):
            total = total + got[d - 1].astype(F32)
        mid[...] = total.astype(BF16)
        for d in range(1, n_in):
            launch(XF + i, mid.at[x_peer(d)], dst.at[d - 1], zf_r.at[i, 1], x_dev(d))

    def zf_final(i, mid, got):
        took(got, zf_r.at[i, 1])
        total = mid[xi].astype(F32)
        for d in range(1, n_in):
            total = total + got[d - 1].astype(F32)
        return total

    def squares_x(i, values):
        ones = jnp.ones((SUBLANES, feats), F32)
        sqx[i, 0] = lax.dot_general(
            ones,
            values * values,
            (((1,), (1,)), ((), ())),
            precision=lax.Precision.HIGHEST,
            preferred_element_type=F32,
        )
        for d in range(1, n_in):
            launch(SQX + i, sqx.at[i, 0], sqx.at[i, d], sq_r.at[i, 0], x_dev(d))

    def squares_z(i):
        if n_in > 1:
            took(sqx.at[i, 1:n_in], sq_r.at[i, 0])
        total = sqx[i, 0]
        for d in range(1, n_in):
            total = total + sqx[i, d]
        sqz[i, 0] = total
        for z, d in z_order:
            launch(SQZ + i, sqz.at[i, 0], sqz.at[i, d], sq_r.at[i, 1], (z * n_in + xi, tp))

    def inverse(i):
        if n_out > 1:
            took(sqz.at[i, 1:n_out], sq_r.at[i, 1])
        total = sqz[i, 0]
        for d in range(1, n_out):
            total = total + sqz[i, d]
        lane = lax.broadcasted_iota(jnp.int32, (rows, batch), 1)
        mine = lax.broadcasted_iota(jnp.int32, (rows, batch), 0) + kv * rows
        own = jnp.where(lane == mine, jnp.broadcast_to(total[:1], (rows, batch)), 0.0)
        return lax.rsqrt(jnp.sum(own, axis=1, keepdims=True) / d_model + eps)

    for load in first_loads:
        load.wait()
    wide = tokens_ref[...].astype(F32)
    scaled = (wide * norm_gain_ref[...].astype(F32).reshape(1, -1)).astype(BF16)

    for k, c in enumerate(order):
        lo, hi = bounds[c]
        took(wall.at[:, lo:hi], w_sem.at[c])
        scatter_rows(px, jnp.dot(scaled, wall[:, lo:hi], preferred_element_type=F32), lo)
        if k == 0:
            pl.semaphore_wait(barrier, len(peers))
        if c == a_zf:
            zf_send(0, px, zfr, lo, hi)
        else:
            send_x(AX, px, rx, fx_r.at[c], lo, hi)
        if k == A_SQ:
            squares_x(0, wide)
    load_decay = fetch(log_decay_hbm, log_decay_ref, in_sem.at[0])
    load_gain = fetch(out_gain_hbm, out_gain_ref, in_sem.at[1])
    load_mixer = fetch(mixer_gain_hbm, mixer_gain_ref, in_sem.at[2])
    load_state = fetch(state_hbm, ns_ref, bulk_sem.at[0])
    load_o = fetch(wo_hbm, wo.at[xi], bulk_sem.at[1])
    fchunks = ff_chunks(ff, FF_Z if two_way else 0)
    n_c = len(fchunks)
    d_zf = n_c - 1 if two_way and n_c > 1 else None
    fbounds = [(2 * lo, 2 * hi) for lo, hi in fchunks]
    for lo, hi in fchunks:
        fetch(wfg_hbm.at[:, lo:hi], wff.at[:, 2 * lo : lo + hi], bulk_sem.at[2])
        fetch(wfu_hbm.at[:, lo:hi], wff.at[:, lo + hi : 2 * hi], bulk_sem.at[2])
    load_dn = fetch(wdn_hbm, wdn, bulk_sem.at[3])

    x_order = [c for c in order if c != a_zf]
    for k, c in enumerate(x_order):
        lo, hi = bounds[c]
        if a_zf is not None and k == len(x_order) - 1:
            zf_to_x(0, px, zfr, zfs, zfx, *bounds[a_zf])
        reduce_x(px, rx, pz, fx_r.at[c], lo, hi)
        send_z(AZ, pz, rz, fz_r.at[c], lo, hi)
        if k == A_SQZ:
            squares_z(0)

    for d in range(1, n_in):
        launch(BX, wo_hbm, wo.at[xi], t_r.at[2], x_dev(d))

    def arrived(c):
        if c == a_zf:
            return zf_final(0, zfs, zfx)
        return reduce_z(pz, rz, fz_r.at[c], *bounds[c])


    load_decay.wait()
    load_state.wait()
    inv = None
    for h in range(heads):
        c = 2 * h
        q_at, k_at, d_at, v_at = (at for at in where[h])
        qk = arrived(c)
        if h == 0:
            inv = inverse(0)
        qk = qk * inv
        dv_terms = arrived(c + 1) * inv
        query = qk[:, :dk] * dk ** (-0.5)
        pre = dv_terms[:, :dk]
        values = dv_terms[:, dk:]
        log_sig = jnp.minimum(pre, 0.0) - jnp.log1p(jnp.exp(-jnp.abs(pre)))
        decay = jnp.exp(log_sig / gate_norm + log_decay_ref[:, h * dk : (h + 1) * dk])
        q_t = query.T
        k_t = qk[:, dk:].T
        a_t = decay.T
        for b in range(rows):
            col = slice(b, b + 1)
            new = ns_ref[b, h] * a_t[:, col] + k_t[:, col] * values[col, :]
            ns_ref[b, h] = new
            att[h, col, :] = jnp.sum(new * q_t[:, col], axis=0, keepdims=True)

    load_gain.wait()
    last = len(bounds) - 1
    gate = reduce_z(pz, rz, fz_r.at[last], *bounds[last]) * inv
    for h in range(heads):
        got = att[h]
        normed = (
            got
            * lax.rsqrt(jnp.mean(got * got, axis=1, keepdims=True) + eps)
            * out_gain_ref[...]
        )
        cols = slice(h * dv, (h + 1) * dv)
        mg[zi, :, cols] = (normed * jax.nn.silu(gate[:, cols])).astype(BF16)

    own = mg.at[zi]
    for z, _ in z_order:
        launch(BZ, own, own, mz_r.at[0], (z * n_in + xi, tp))
    load_o.wait()
    if n_in > 1:
        took(wo.at[: n_in - 1], t_r.at[2])
    if n_out > 1:
        took(mg.at[: n_out - 1], mz_r.at[0])
    mixed = mg[...].reshape(n_out * rows, vw)
    mine = xi * n_tp + tp
    for d in range(1, n_in):
        part = jnp.dot(mixed, wo[x_peer(d)], preferred_element_type=F32)
        away[d - 1] = part.astype(BF16)
        for e in range(n_tp):
            launch(CY, away.at[d - 1], to.at[mine], t_r.at[3], xt_dev(d, e))
    to[mine] = jnp.dot(mixed, wo[xi], preferred_element_type=F32).astype(BF16)
    for e in range(1, n_tp):
        launch(CY, to.at[mine], to.at[mine], t_r.at[0], t_dev(e))

    def heads_sum(x):
        total = to[x * n_tp].astype(F32)
        for g in range(1, n_tp):
            total = total + to[x * n_tp + g].astype(F32)
        tok = jnp.stack(
            [tokens_ref[pl.ds((z * n_in + x) * rows, rows), :] for z in range(n_out)]
        )
        return (tok.astype(F32) + total.reshape(n_out, rows, feats)).astype(BF16)

    if n_tp > 1:
        took(to.at[: n_tp - 1], t_r.at[0])
    middle_ref[:, xi] = heads_sum(xi)
    if n_in > 1:
        took(to.at[: (n_in - 1) * n_tp], t_r.at[3])
    for d in range(1, n_in):
        middle_ref[:, x_peer(d)] = heads_sum(x_peer(d))
    middle = middle_ref[...].reshape(batch, feats)

    def sum_groups(phase, buf, sem):
        for d in range(1, n_tp):
            launch(phase, buf.at[tp], buf.at[tp], sem, t_dev(d))
        if n_tp > 1:
            took(buf.at[: n_tp - 1], sem)
        total = buf[0].astype(F32)
        for g in range(1, n_tp):
            total = total + buf[g].astype(F32)
        return total

    load_mixer.wait()
    wide2 = middle.astype(F32)
    scaled2 = (wide2 * mixer_gain_ref[...].astype(F32).reshape(1, -1)).astype(BF16)
    took(wff, bulk_sem.at[2])
    d_order = list(range(n_c))
    if d_zf is not None:
        d_order = [0, d_zf] + list(range(1, d_zf))
    for k, c in enumerate(d_order):
        lo, hi = fbounds[c]
        scatter_rows(fx, jnp.dot(scaled2, wff[:, lo:hi], preferred_element_type=F32), lo)
        if c == d_zf:
            zf_send(1, fx, dfr, lo, hi)
        else:
            send_x(DX, fx, frx, fx_r.at[c], lo, hi)
        if k == min(SQ_AT, n_c - 1):
            squares_x(1, wide2)

    inv2 = [None]

    def to_z(c):
        lo, hi = fbounds[c]
        reduce_x(fx, frx, fz, fx_r.at[c], lo, hi)
        send_z(DZ, fz, frz, fz_r.at[c], lo, hi)
        if c == SQ_Z:
            squares_z(1)

    def activate(c):
        if c == d_zf:
            terms = zf_final(1, dfs, dfx)
        else:
            terms = reduce_z(fz, frz, fz_r.at[c], *fbounds[c])
        if inv2[0] is None:
            inv2[0] = inverse(1)
        terms = terms * inv2[0]
        fc = terms.shape[1] // 2
        cols = slice(*fchunks[c])
        hg[zi, xi, :, cols] = (jax.nn.silu(terms[:, :fc]) * terms[:, fc:]).astype(BF16)
        own = hg.at[zi, xi, :, cols]
        for z, _ in z_order:
            launch(EZ, own, own, fx_r.at[c], (z * n_in + xi, tp))
        for d in range(1, n_in):
            launch(EX, own, own, hx_r.at[c], x_dev(d))
            if direct(c):
                for z, _ in z_order:
                    launch(EX, own, own, hx_r.at[c], (z * n_in + x_peer(d), tp))

    def direct(c):
        return n_c - 1 - DIRECT <= c < n_c - 1

    def hand_on(c):
        cols = slice(*fchunks[c])
        if n_out > 1:
            took(hg.at[: n_out - 1, 0, :, cols], fx_r.at[c])
        if direct(c):
            return
        for d in range(1, n_in):
            for z in range(1, n_out):
                slot = hg.at[z_back(z), xi, :, cols]
                launch(EX, slot, slot, hx_r.at[c], x_dev(d))

    steps = []
    for c in range(n_c):
        at = fchunks[c][1] / LANES
        if c == d_zf:
            steps.append((LAG_ZX, len(steps), lambda c: zf_to_x(1, fx, dfr, dfs, dfx, *fbounds[c]), c))
            steps.append((LAG_ZACT, len(steps), activate, c))
        else:
            steps.append((at, len(steps), to_z, c))
            steps.append((at + LAG_ACT, len(steps), activate, c))
        steps.append((at + LAG_HAND if c != d_zf else LAG_ZHAND, len(steps), hand_on, c))
    for _, _, step, c in sorted(steps, key=lambda item: item[:2]):
        step(c)

    load_dn.wait()
    down = None
    for c, (lo, hi) in enumerate(fchunks):
        if n_in > 1:
            took(hg.at[:, : n_in - 1, :, lo:hi], hx_r.at[c])
        term = jnp.dot(
            hg[:, :, :, lo:hi].reshape(batch, hi - lo),
            wdn[lo:hi, :],
            preferred_element_type=F32,
        )
        down = term if down is None else down + term
    td[tp] = down.astype(BF16)
    total = sum_groups(FY, td, t_r.at[1])
    wide3 = middle_ref[...].reshape(batch, feats).astype(F32)
    result_ref[...] = (wide3 + total).astype(BF16)

    def sent_but(ref, phase, ranges, but):
        left = sum(hi - lo for c, (lo, hi) in enumerate(ranges) if c != but)
        took(ref.at[..., :left], send_sem.at[phase])

    if a_zf is not None:
        took(zfr, send_sem.at[ZF])
        took(zfx, send_sem.at[XF])
    if d_zf is not None:
        took(dfr, send_sem.at[ZF + 1])
        took(dfx, send_sem.at[XF + 1])
    if n_in > 1:
        sent_but(rx, AX, bounds, a_zf)
        sent_but(frx, DX, fbounds, d_zf)
        took(wo.at[: n_in - 1], send_sem.at[BX])
        took(hg.at[:, : n_in - 1], send_sem.at[EX])
        for i in range(2):
            took(sqx.at[i, 1:n_in], send_sem.at[SQX + i])
    if n_out > 1:
        sent_but(rz, AZ, bounds, a_zf)
        sent_but(frz, DZ, fbounds, d_zf)
        took(mg.at[: n_out - 1], send_sem.at[BZ])
        took(hg.at[: n_out - 1, 0], send_sem.at[EZ])
        for i in range(2):
            took(sqz.at[i, 1:n_out], send_sem.at[SQZ + i])
    if n_in * n_tp > 1:
        took(to.at[: n_in * n_tp - 1], send_sem.at[CY])
    if n_tp > 1:
        took(td.at[: n_tp - 1], send_sem.at[FY])


def body(n_kv, n_tp, *args):
    (
        tokens,
        norm_gain,
        w_query,
        w_key,
        w_value,
        w_gate,
        w_decay,
        log_decay,
        state,
        out_gain,
        w_out,
        mixer_gain,
        w_ffgate,
        w_ffup,
        w_down,
    ) = args
    n_out, n_in = split_axis(n_kv)
    batch, feats = tokens.shape
    rows, heads, dk, dv = state.shape
    kw = w_query.shape[1]
    vw = w_value.shape[1]
    ff = w_ffgate.shape[1]
    n_in_out = n_in > 1 and n_out > 1
    fchunks = ff_chunks(ff, FF_Z if n_in_out else 0)
    n_c = len(fchunks)
    d_w = 2 * (fchunks[-1][1] - fchunks[-1][0])
    a_w = 2 * dk
    chunks, _, _, width = proj_layout(kw, vw, dk, dv)
    n_a = len(chunks)
    m_in, m_out = max(n_in - 1, 1), max(n_out - 1, 1)
    dma = pltpu.SemaphoreType.DMA
    vmem = pltpu.VMEM
    whole = pl.BlockSpec(memory_space=pltpu.VMEM)
    far = pl.BlockSpec(memory_space=pl.ANY)
    sems = [
        (3,),
        (n_a,),
        (4,),
        (PHASES,),
        (2, 2),
        (1,),
        (4,),
        (max(n_a, n_c),),
        (max(n_a, n_c),),
        (n_c,),
        (2, 2),
    ]
    result, new_state = pl.pallas_call(
        functools.partial(kernel, n_kv, n_tp, feats * n_kv),
        out_shape=(
            vmem((batch, feats), BF16),
            vmem(state.shape, F32),
        ),
        in_specs=[far] * 15,
        out_specs=(whole, whole),
        scratch_shapes=[
            vmem((batch, feats), BF16),
            vmem(norm_gain.shape, BF16),
            vmem(log_decay.shape, F32),
            vmem((1, dv), F32),
            vmem(mixer_gain.shape, BF16),
            vmem((feats, width), BF16),
            vmem((n_in,) + w_out.shape, BF16),
            vmem((feats, 2 * ff), BF16),
            vmem(w_down.shape, BF16),
            vmem((2, n_in, SUBLANES, batch), F32),
            vmem((2, n_out, SUBLANES, batch), F32),
            vmem((n_in, n_out, rows, width), BF16),
            vmem((m_in, n_out, rows, width), BF16),
            vmem((n_out, rows, width), BF16),
            vmem((m_out, rows, width), BF16),
            vmem((heads, rows, dv), F32),
            vmem((n_out, rows, vw), BF16),
            vmem((n_in * n_tp, n_out * rows, feats), BF16),
            vmem((m_in, n_out * rows, feats), BF16),
            vmem((n_in, n_out, rows, 2 * ff), BF16),
            vmem((m_in, n_out, rows, 2 * ff), BF16),
            vmem((n_out, rows, 2 * ff), BF16),
            vmem((m_out, rows, 2 * ff), BF16),
            vmem((n_out, n_in, rows, ff), BF16),
            vmem((n_tp, batch, feats), BF16),
            vmem((n_out, n_in, rows, feats), BF16),
            vmem((m_out, n_in, rows, a_w), BF16),
            vmem((n_in, rows, a_w), BF16),
            vmem((m_in, rows, a_w), BF16),
            vmem((m_out, n_in, rows, d_w), BF16),
            vmem((n_in, rows, d_w), BF16),
            vmem((m_in, rows, d_w), BF16),
        ]
        + [dma(shape) for shape in sems],
        compiler_params=pltpu.CompilerParams(
            collective_id=0, has_side_effects=True, vmem_limit_bytes=56 * 2**20
        ),
    )(
        tokens,
        norm_gain,
        w_query,
        w_key,
        w_value,
        w_gate,
        w_decay,
        log_decay,
        state,
        out_gain.reshape(1, dv),
        w_out,
        mixer_gain,
        w_ffgate,
        w_ffup,
        w_down,
    )
    return (result, new_state)


def solution(mesh):
    return jax.shard_map(
        functools.partial(body, mesh.shape["kv"], mesh.shape["tp"]),
        mesh=mesh,
        in_specs=(
            P(None, "kv"),
            P("kv"),
            P("kv", "tp"),
            P("kv", "tp"),
            P("kv", "tp"),
            P("kv", "tp"),
            P("kv", "tp"),
            P("kv", "tp"),
            P("kv", "tp", None, None),
            P(),
            P("tp", "kv"),
            P("kv"),
            P("kv", "tp"),
            P("kv", "tp"),
            P("tp", "kv"),
        ),
        out_specs=(P(None, "kv"), P("kv", "tp", None, None)),
        check_vma=False,
    )
```
